32 devices in a mesh: sp: 4 (over z), tp: 4 (over y, x), dp: 2 (over core).
Axes of the slice: x: 2, y: 2, z: 4, core: 2. Of those that a mesh axis runs over, the one named last changes fastest.
Arguments:
- latent: bfloat16 [2, 1024, 2048], P('dp', 'sp'), may hold values from -1.5 to 1.5
- condition: bfloat16 [2, 2048], P('dp', 'sp'), may hold values from -6 to 6
- context: bfloat16 [2, 1024, 2048], P('dp', 'sp'), may hold values from -6 to 6
- context_code: bfloat16 [2048], P('sp'), may hold values from -6 to 6
- shift_weight: bfloat16 [2048, 2048], P('sp', 'tp'), may hold values from -0.125 to 0.125
- scale_weight: bfloat16 [2048, 2048], P('sp', 'tp'), may hold values from -0.125 to 0.125
- gate_weight: bfloat16 [2048, 2048], P('sp', 'tp'), may hold values from -0.125 to 0.125
- norm_gain: float32 [2048], replicated, may hold values from 0.1 to 1.9
- query_weight: bfloat16 [2048, 1024], P(None, 'tp'), may hold values from -0.125 to 0.125
- key_weight: bfloat16 [2048, 256], P(None, 'tp'), may hold values from -0.125 to 0.125
- value_weight: bfloat16 [2048, 256], P(None, 'tp'), may hold values from -0.125 to 0.125
- output_weight: bfloat16 [1024, 2048], P('tp'), may hold values from -0.75 to 0.75
- query_gain: float32 [64], replicated, may hold values from 1 to 5.5
- key_gain: float32 [64], replicated, may hold values from 1 to 5.5
- context_bias: float32 [16], P('tp'), may hold values from 0.5 to 2
Outputs:
- updated: bfloat16 [2, 1024, 2048], P('dp', 'sp')
The draws below stay inside these ranges and needn't reach their ends.
All inputs are finite; a program needn't handle non-finite values.
Results may differ from the reference program's by a relative error of at most 0.01405.
The reference program's roundings to bfloat16 on the way count: a program that leaves them out, or rounds other values in their place, can miss the bound.
Values may be sent and summed in bfloat16 or wider, within the bound.
A program may use at most 64 MiB of HBM per device.

```python
import math
import jax
import jax.numpy as jnp
from jax import lax

D = 2048
HEADS = 16
KV_HEADS = 4
HEAD = 64
GRID_W = 64
CTX = 1024
SAMPLES = 2
SEQ = 1024


def gain_draw(key, salt):
    fresh = jax.random.fold_in(key, salt)
    return jnp.exp(jax.random.uniform(fresh, (HEAD,), jnp.float32, 0.0, math.log(2.2)))


def draw_query_gain(key, part):
    return gain_draw(key, 17)


def draw_key_gain(key, part):
    return gain_draw(key, 29)


def shard_levels(rng, dims, cuts, smallest, largest):
    gain, own = 1.0, jax.random.fold_in(rng, 6)
    for dim, blocks in cuts:
        draws = jnp.exp(jax.random.uniform(jax.random.fold_in(own, dim), (blocks,), jnp.float32, smallest / len(cuts), largest / len(cuts)))
        gain = gain * jnp.repeat(draws, dims[dim] // blocks).reshape([-1 if axis == dim else 1 for axis in range(len(dims))])
    return gain


def centred(stream_key, dims, spread, bound, split=(), kind=jnp.bfloat16):
    entries = spread * jax.random.normal(stream_key, dims, jnp.float32)
    if split:
        entries = entries * shard_levels(stream_key, dims, split, -0.22, 0.18)
    return jnp.clip(entries, -bound, bound).astype(kind)


def setup_inputs(seed: int = 0) -> dict:
    key_of = jax.random.split(jax.random.key(seed), 16)
    latent = centred(key_of[0], (SAMPLES, SEQ, D), 0.25, 1.5, ((0, 2), (1, 4)))
    condition = centred(key_of[1], (SAMPLES, D), 1.0, 6.0, ((0, 2), (1, 4)))
    context = centred(key_of[2], (SAMPLES, CTX, D), 1.0, 6.0, ((0, 2), (1, 4)))
    context_code = centred(key_of[3], (D,), 1.0, 6.0, ((0, 4),))
    shift_weight = centred(key_of[4], (D, D), D ** -0.5, 0.125, ((0, 4), (1, 4)))
    scale_weight = centred(key_of[5], (D, D), D ** -0.5, 0.125, ((0, 4), (1, 4)))
    gate_weight = centred(key_of[6], (D, D), D ** -0.5, 0.125, ((0, 4), (1, 4)))
    norm_gain = jnp.clip(1.0 + 0.18 * jax.random.normal(key_of[7], (D,), jnp.float32), 0.1, 1.9)
    query_weight = centred(key_of[8], (D, HEADS * HEAD), D ** -0.5, 0.125, ((1, 4),))
    key_weight = centred(key_of[9], (D, KV_HEADS * HEAD), D ** -0.5, 0.125, ((1, 4),))
    value_weight = centred(key_of[10], (D, KV_HEADS * HEAD), D ** -0.5, 0.125, ((1, 4),))
    output_weight = centred(key_of[11], (HEADS * HEAD, D), (HEADS * HEAD // 16) ** -0.5, 0.75, ((0, 4),))
    query_gain = draw_query_gain(jax.random.fold_in(key_of[15], 71), 0)
    key_gain = draw_key_gain(jax.random.fold_in(key_of[15], 71), 0)
    context_bias = jnp.clip(0.5 + 1.5 * jax.random.uniform(key_of[14], (HEADS,), jnp.float32) ** shard_levels(key_of[14], (HEADS,), ((0, 4),), -0.2, 0.2), 0.5, 2.0)
    return {"latent": latent, "condition": condition, "context": context, "context_code": context_code, "shift_weight": shift_weight, "scale_weight": scale_weight, "gate_weight": gate_weight, "norm_gain": norm_gain, "query_weight": query_weight, "key_weight": key_weight, "value_weight": value_weight, "output_weight": output_weight, "query_gain": query_gain, "key_gain": key_gain, "context_bias": context_bias}


norm_eps = 1e-06
rope_base = 10000.0

def rotary_tables(position):
    grid_row = (position // GRID_W).astype(jnp.float32)
    grid_col = (position % GRID_W).astype(jnp.float32)
    quarter = HEAD // 4
    inverse = rope_base ** (-jnp.arange(quarter, dtype=jnp.float32) / quarter)
    angles = jnp.concatenate([grid_row[:, None] * inverse, grid_col[:, None] * inverse], axis=-1)
    return (jnp.cos(angles), jnp.sin(angles))

def head_norm(values, gain_row):
    return values * lax.rsqrt(lax.optimization_barrier(jnp.mean(values * values, axis=-1, keepdims=True)) + norm_eps) * gain_row

def rotate(values, cosine, sine_part):
    half_dim = values.shape[-1] // 2
    first_half = values[..., :half_dim]
    second_half = values[..., half_dim:]
    cos_rows = cosine[:, None, :]
    sin_rows = sine_part[:, None, :]
    return jnp.concatenate([first_half * cos_rows - second_half * sin_rows, second_half * cos_rows + first_half * sin_rows], axis=-1)

def modulated(tokens, gain_row, shift_row, scale_row):
    floats = tokens.astype(jnp.float32)
    normal = floats * lax.rsqrt(lax.optimization_barrier(jnp.mean(floats * floats, axis=-1, keepdims=True)) + norm_eps)
    return (normal * gain_row * (1.0 + scale_row) + shift_row).astype(jnp.bfloat16)

def attend(query_block, latent_keys, latent_values, context_keys, context_values, bias_value):
    score_scale = HEAD ** (-0.5)
    latent_scores = jnp.dot(query_block, latent_keys.T, preferred_element_type=jnp.float32) * score_scale
    context_scores = jnp.dot(query_block, context_keys.T, preferred_element_type=jnp.float32) * score_scale + bias_value
    row_max = jnp.maximum(latent_scores.max(axis=1), context_scores.max(axis=1))[:, None]
    latent_exp = jnp.exp(latent_scores - row_max)
    context_exp = jnp.exp(context_scores - row_max)
    totals = latent_exp.sum(axis=1) + context_exp.sum(axis=1)
    summed = jnp.dot(latent_exp.astype(jnp.bfloat16), latent_values, preferred_element_type=jnp.float32)
    summed = summed + jnp.dot(context_exp.astype(jnp.bfloat16), context_values, preferred_element_type=jnp.float32)
    return (summed / totals[:, None]).astype(jnp.bfloat16)

def reference(latent, condition, context, context_code, shift_weight, scale_weight, gate_weight, norm_gain, query_weight, key_weight, value_weight, output_weight, query_gain, key_gain, context_bias):
    cosine, sine_part = rotary_tables(jnp.arange(SEQ, dtype=jnp.int32))
    group_size = HEADS // KV_HEADS
    query_block = math.gcd(SEQ, 512)
    context_act = jax.nn.silu(context_code.astype(jnp.float32)).astype(jnp.bfloat16)
    context_shift = jnp.dot(context_act, shift_weight, preferred_element_type=jnp.float32)
    context_scale = jnp.dot(context_act, scale_weight, preferred_element_type=jnp.float32)
    results = []
    for sample in range(SAMPLES):
        activated = jax.nn.silu(condition[sample].astype(jnp.float32)).astype(jnp.bfloat16)
        latent_shift = jnp.dot(activated, shift_weight, preferred_element_type=jnp.float32)
        latent_scale = jnp.dot(activated, scale_weight, preferred_element_type=jnp.float32)
        latent_gate = jnp.dot(activated, gate_weight, preferred_element_type=jnp.float32)
        normed = modulated(latent[sample], norm_gain, latent_shift, latent_scale)
        queries = jnp.dot(normed, query_weight, preferred_element_type=jnp.float32).reshape(SEQ, HEADS, HEAD)
        queries = rotate(head_norm(queries, query_gain), cosine, sine_part).astype(jnp.bfloat16)
        latent_keys = jnp.dot(normed, key_weight, preferred_element_type=jnp.float32).reshape(SEQ, KV_HEADS, HEAD)
        latent_keys = rotate(head_norm(latent_keys, key_gain), cosine, sine_part).astype(jnp.bfloat16)
        latent_values = jnp.dot(normed, value_weight, preferred_element_type=jnp.float32)
        latent_values = latent_values.reshape(SEQ, KV_HEADS, HEAD).astype(jnp.bfloat16)
        context_normed = modulated(context[sample], norm_gain, context_shift, context_scale)
        context_keys = jnp.dot(context_normed, key_weight, preferred_element_type=jnp.float32).reshape(CTX, KV_HEADS, HEAD)
        context_keys = head_norm(context_keys, key_gain).astype(jnp.bfloat16)
        context_values = jnp.dot(context_normed, value_weight, preferred_element_type=jnp.float32)
        context_values = context_values.reshape(CTX, KV_HEADS, HEAD).astype(jnp.bfloat16)
        mixed = jnp.zeros((SEQ, D), jnp.float32)
        for kv_head in range(KV_HEADS):
            outputs = []
            for head_index in range(kv_head * group_size, (kv_head + 1) * group_size):
                head_out = lax.map(partial_attend(latent_keys[:, kv_head], latent_values[:, kv_head], context_keys[:, kv_head], context_values[:, kv_head], context_bias[head_index]), queries[:, head_index].reshape(SEQ // query_block, query_block, HEAD))
                outputs.append(head_out.reshape(SEQ, HEAD))
            attended = jnp.concatenate(outputs, axis=1)
            rows_start = kv_head * group_size * HEAD
            weight_rows = output_weight[rows_start:rows_start + group_size * HEAD]
            partial_sum = jnp.dot(attended, weight_rows, preferred_element_type=jnp.float32).astype(jnp.bfloat16)
            mixed = mixed + partial_sum.astype(jnp.float32)
        updated = latent[sample].astype(jnp.float32) + latent_gate * mixed
        results.append(updated.astype(jnp.bfloat16))
    return jnp.stack(results)

def partial_attend(latent_keys, latent_values, context_keys, context_values, bias_value):

    def attend_block(query_block):
        return attend(query_block, latent_keys, latent_values, context_keys, context_values, bias_value)
    return attend_block
```

```python
import functools
import math

import jax
import jax.numpy as jnp
from jax import lax
from jax.experimental import pallas as pl
from jax.experimental.pallas import tpu as pltpu
from jax.sharding import PartitionSpec as P

GRID_W = 64
norm_eps = 1e-06
rope_base = 10000.0
F32 = jnp.float32
BF16 = jnp.bfloat16
LANES = 128
LOG2E = math.log2(math.e)
PARTS = 4
SCOPED_KIB = 64384


def tables(first, rows, head_dim):
    quarter = head_dim // 4
    half = head_dim // 2
    shape = (rows, 2 * head_dim)
    token = first + lax.broadcasted_iota(jnp.int32, shape, 0)
    lane = lax.broadcasted_iota(jnp.int32, shape, 1) % head_dim
    pair = lane % half
    index = (pair % quarter).astype(F32)
    place = jnp.where(pair < quarter, token // GRID_W, token % GRID_W).astype(F32)
    angle = place * jnp.exp(index * (-math.log(rope_base) / quarter))
    sine = jnp.sin(angle)
    return jnp.cos(angle), jnp.where(lane < half, -sine, sine)


def kernel(
    sizes,
    condition, code, gain_ref, q_gain, k_gain, bias_ref,
    latent, context, shift_w, scale_w, gate_w, wq, wk, wv, wo,
    out,
    modw, lat, ctx, wq_v, wkv, wbuf,
    vec_z, vec_t, gate_z, gate_t, normed, kvbuf, vals, q_s, m_s, acc, att, mixed, cos_s, sin_s, inv_s,
    local, met,
    z_send, z_recv, t_send, t_recv, gz_send, gz_recv, gt_send, gt_recv, kv_send, kv_recv,
    w_send, w_recv, f_send, f_recv, a_send, a_recv,
):
    n_sp, n_tp, n_dp = sizes
    sp, tp, dp = lax.axis_index("sp"), lax.axis_index("tp"), lax.axis_index("dp")
    rows, crows = lat.shape[0], ctx.shape[0]
    hd = wk.shape[0]
    qcols = wq_v.shape[1]
    heads = qcols // hd
    width = lat.shape[1]
    cols = width // n_tp
    side = cols // 2
    chip = cols // 4
    mid = rows // 2
    lanes = 2 * hd
    dots = functools.partial(jnp.dot, preferred_element_type=F32)
    dims = (((1,), (1,)), ((), ()))
    scope = jax.named_scope

    copies = {}
    for number, (name, src, dst) in enumerate((
        ("m0", shift_w, modw.at[0]), ("m1", scale_w, modw.at[1]),
        ("ctx", context.at[0], ctx), ("wk", wk, wkv.at[:hd]), ("wv", wv, wkv.at[hd:]),
        ("m2", gate_w, modw.at[2]), ("lat", latent.at[0], lat),
        ("wq", wq, wq_v), ("wo", wo, wbuf.at[tp]),
    )):
        copies[name] = pltpu.make_async_copy(src, dst, local.at[number])
        copies[name].start()

    barrier = pltpu.get_barrier_semaphore()

    def greet(sem, **where):
        pl.semaphore_signal(sem, inc=1, device_id=where, device_id_type=pl.DeviceIdType.MESH)

    for d in range(1, n_sp):
        greet(barrier, sp=(sp + d) % n_sp)
    for d in range(1, n_tp):
        greet(barrier, tp=tp ^ d)
    for d in range(1, n_dp):
        @pl.when(dp + d < n_dp)
        def _():
            greet(barrier, dp=dp + d)

    def remote(src, dst, s, r, **where):
        return pltpu.make_async_remote_copy(
            src_ref=src, dst_ref=dst, send_sem=s, recv_sem=r,
            device_id=where, device_id_type=pl.DeviceIdType.MESH)

    with scope("modmat"):
        row8 = lax.broadcasted_iota(jnp.int32, (8, condition.shape[1]), 0)
        own_code = condition[...].astype(F32)
        shared_code = code[...].astype(F32)[None]
        both = jnp.where(row8 == 0, own_code, jnp.where(row8 == 1, shared_code, 0.0))
        both = (both / (1.0 + jnp.exp(-both))).astype(BF16)
        pieces = []
        for k in range(2):
            copies[f"m{k}"].wait()
            pieces.append(dots(both, modw[k])[:2])
        rows4 = jnp.concatenate(pieces, axis=0)
        vec_z[sp] = jnp.concatenate([rows4[:, :side], rows4[:, side:]], axis=0)

    with scope("barrier"):
        pl.semaphore_wait(barrier, n_sp + n_tp - 2 + dp)

    z_copies = []
    for d in range(1, n_sp):
        copy = remote(vec_z.at[sp], vec_z.at[sp], z_send.at[d], z_recv.at[d], sp=(sp + d) % n_sp)
        copy.start()
        z_copies.append(copy)
    for d in range(1, n_dp):
        @pl.when(dp - d >= 0)
        def _():
            greet(met, dp=dp - d)

    share = wo.shape[0] // n_dp
    piece = share // PARTS
    near = [d for d in (1, 2) if d < n_tp]
    turns = {1: (2, 3, 0, 1), 2: (0, 1, 2, 3)}
    waiting = []

    def span(core, part):
        return pl.ds(core * share + part * piece, piece)

    def send_weights(turn):
        for d in near:
            part = turns[d][turn]
            copy = remote(wo.at[span(dp, part)], wbuf.at[tp, span(dp, part)],
                          w_send.at[d, part], w_recv.at[d, part], tp=tp ^ d)
            copy.start()
            waiting.append(copy)

    def got_weights(d, part):
        ref = wbuf.at[tp ^ d, span(dp, part)]
        remote(ref, ref, w_send.at[d, part], w_recv.at[d, part], tp=tp ^ d).wait_recv()
        if n_tp == 4 and d < 3 and part in turns[d][:2]:
            copy = remote(ref, ref, w_send.at[3, part], w_recv.at[3, part], tp=tp ^ (3 - d))
            copy.start()
            waiting.append(copy)
        for e in range(1, n_dp):
            copy = remote(ref, ref, f_send.at[d, part, e], f_recv.at[d, part, e], dp=(dp + e) % n_dp)
            copy.start()
            waiting.append(copy)

    send_weights(0)

    with scope("gate"):
        copies["m2"].wait()
        row = dots(both, modw[2])[:1]
        gate_z[sp] = jnp.concatenate([row[:, j * chip:(j + 1) * chip] for j in range(4)], axis=0)
    g_copies = []
    for d in range(1, n_sp):
        copy = remote(gate_z.at[sp], gate_z.at[sp], gz_send.at[d], gz_recv.at[d], sp=(sp + d) % n_sp)
        copy.start()
        g_copies.append(copy)

    with scope("tables"):
        cosine, sine = tables(sp * rows, rows, hd)
        cos_s[...] = cosine
        sin_s[...] = sine
    with scope("inv"):
        copies["ctx"].wait()
        floats = ctx[...].astype(F32)
        inv_c = lax.rsqrt(jnp.mean(floats * floats, axis=-1, keepdims=True) + norm_eps)
        copies["lat"].wait()
        floats = lat[...].astype(F32)
        inv_s[...] = lax.rsqrt(jnp.mean(floats * floats, axis=-1, keepdims=True) + norm_eps)

    with scope("zwait"):
        for copy in z_copies:
            copy.wait()
    total = vec_z[0]
    for k in range(1, n_sp):
        total = total + vec_z[k]
    vec_t[tp] = total
    for d in reversed(range(1, n_tp)):
        copy = remote(vec_t.at[tp], vec_t.at[tp], t_send.at[d], t_recv.at[d], tp=tp ^ d)
        copy.start()
        waiting.append(copy)
    for turn in range(1, PARTS):
        send_weights(turn)
    with scope("twait"):
        for d in range(1, n_tp):
            remote(vec_t.at[tp ^ d], vec_t.at[tp ^ d], t_send.at[d], t_recv.at[d], tp=tp ^ d).wait_recv()

    def modulate(tokens, inverse, which):
        for t in range(n_tp):
            for k in range(2):
                part = slice(t * cols + k * side, t * cols + (k + 1) * side)
                at = 4 * k + which
                factor = gain_ref[:, part] * (1.0 + vec_t[t, at + 2:at + 3, :])
                shift = vec_t[t, at:at + 1, :]
                normed[:tokens.shape[0], part] = (tokens[:, part].astype(F32) * inverse * factor + shift).astype(BF16)

    def kv_copy(block, target, way, part):
        area = pl.ds(0, crows) if part == 0 else pl.ds(crows, rows)
        ref = kvbuf.at[block, area]
        return remote(ref, ref, kv_send.at[way, part, block], kv_recv.at[part, block], sp=target)

    def send_own(part):
        @pl.when(sp + 1 < n_sp)
        def _():
            kv_copy(sp, sp + 1, 0, part).start()

        @pl.when(sp > 0)
        def _():
            kv_copy(sp, sp - 1, 1, part).start()

    def averages(values):
        n = values.shape[1]
        row = lax.broadcasted_iota(jnp.int32, (n, n), 0) // hd
        col = lax.broadcasted_iota(jnp.int32, (n, n), 1) // hd
        spread = jnp.where(row == col, 1.0 / hd, 0.0).astype(BF16)
        return dots((values * values).astype(BF16), spread)

    def swapped(values):
        lane = lax.broadcasted_iota(jnp.int32, values.shape, 1) % hd
        return jnp.where(lane < hd // 2, pltpu.roll(values, lanes - hd // 2, 1), pltpu.roll(values, hd // 2, 1))

    def key_values(count, turn):
        kv = lax.dot_general(normed[:count], wkv[...], dims, preferred_element_type=F32)
        lane = lax.broadcasted_iota(jnp.int32, kv.shape, 1)
        keys = kv * lax.rsqrt(averages(kv) + norm_eps) * jnp.concatenate([k_gain[...]] * 2, axis=1)
        if turn:
            keys = keys * cos_s[...] + swapped(keys) * sin_s[...]
        return jnp.where(lane < hd, keys, kv).astype(BF16)

    with scope("modctx"):
        modulate(ctx, inv_c, 1)
    with scope("kvctx"):
        copies["wk"].wait()
        copies["wv"].wait()
        kvbuf[sp, :crows] = key_values(crows, False)
    send_own(0)

    with scope("modlat"):
        modulate(lat, inv_s[...], 0)
    with scope("kvlat"):
        kvbuf[sp, crows:] = key_values(rows, True)
    send_own(1)

    with scope("gotw0"):
        for d in range(1, n_dp):
            @pl.when(dp + d < n_dp)
            def _():
                pl.semaphore_wait(met, 1)
        for d in near:
            got_weights(d, turns[d][0])

    with scope("qproj"):
        copies["wq"].wait()
        queries = dots(normed[:rows], wq_v[...])
        factor = lax.rsqrt(averages(queries) + norm_eps)
        gains = jnp.concatenate([q_gain[...]] * 2, axis=1) * (hd ** -0.5 * LOG2E)
        lane = lax.broadcasted_iota(jnp.int32, (rows, lanes), 1)
        for g in range(heads // 2):
            pair = slice(g * lanes, (g + 1) * lanes)
            two = queries[:, pair] * factor[:, pair] * gains
            two = two * cos_s[...] + swapped(two) * sin_s[...]
            for h, one in ((2 * g, two), (2 * g + 1, pltpu.roll(two, hd, 1))):
                one = jnp.where(lane < hd, one, 0.0).astype(BF16)
                for half in range(2):
                    q_s[half, h * mid:(h + 1) * mid] = one[half * mid:(half + 1) * mid]

    with scope("gatez"):
        for copy in g_copies:
            copy.wait()
        total = gate_z[0]
        for k in range(1, n_sp):
            total = total + gate_z[k]
        gate_t[tp] = total
    for d in range(1, n_tp):
        copy = remote(gate_t.at[tp], gate_t.at[tp], gt_send.at[d], gt_recv.at[d], tp=tp ^ d)
        copy.start()
        waiting.append(copy)

    def spread(column, count):
        if count % LANES == 0:
            return jnp.concatenate([column] * (count // LANES), axis=1)
        return column[:, :count]

    def prepare(block):
        pairs = kvbuf[block]
        lane = lax.broadcasted_iota(jnp.int32, pairs.shape, 1)
        vals[...] = jnp.where(lane < hd, jnp.ones_like(pairs), pairs)

    def absorb(block, half, first=False):
        def scores(h):
            query = q_s[half, h * mid:(h + 1) * mid]
            return (lax.dot_general(query, kvbuf[block, :crows], dims, preferred_element_type=F32),
                    lax.dot_general(query, kvbuf[block, crows:], dims, preferred_element_type=F32))

        ahead = scores(0)
        for h in range(heads):
            s_c, s_l = ahead
            if h + 1 < heads:
                ahead = scores(h + 1)
            bias = bias_ref[h] * LOG2E
            top = jnp.maximum(s_c.max(axis=1, keepdims=True) + bias, s_l.max(axis=1, keepdims=True))
            top = jnp.broadcast_to(top, (mid, lanes))
            new = top if first else jnp.maximum(m_s[half, h], top)
            p_c = jnp.exp2(s_c - spread(new - bias, crows)).astype(BF16)
            p_l = jnp.exp2(s_l - spread(new, rows)).astype(BF16)
            more = dots(p_c, vals[:crows]) + dots(p_l, vals[crows:])
            if first:
                acc[half, h] = more
            else:
                acc[half, h] = acc[half, h] * jnp.exp2(m_s[half, h] - new) + more
            m_s[half, h] = new

    def absorb_all(block, first=False):
        prepare(block)

        @pl.loop(0, 2)
        def _(half):
            absorb(block, half, first)

    with scope("absorb0"):
        absorb_all(sp, True)

    with scope("gotw1"):
        for d in near:
            got_weights(d, turns[d][1])

    last = jnp.where(2 * sp < n_sp, n_sp - 1, 0)

    def forward(s):
        for part in range(2):
            @pl.when(sp - s >= 0)
            def _():
                kv_copy(sp - s, sp, 0, part).wait_recv()

                @pl.when(sp + 1 < n_sp)
                def _():
                    kv_copy(sp - s, sp + 1, 0, part).start()

            @pl.when(sp + s < n_sp)
            def _():
                kv_copy(sp + s, sp, 1, part).wait_recv()

                @pl.when(sp > 0)
                def _():
                    kv_copy(sp + s, sp - 1, 1, part).start()

    @pl.loop(1, n_sp)
    def _(s):
        with scope("fwd"):
            forward(s)

        @pl.loop(0, 2)
        def _(way):
            block = sp + s * (2 * way - 1)

            @pl.when((block >= 0) & (block < n_sp) & (block != last))
            def _():
                with scope("absorb"):
                    absorb_all(block)

    if n_sp > 1:
        with scope("prepare"):
            prepare(last)
    lane = lax.broadcasted_iota(jnp.int32, (mid, lanes), 1)
    for half in range(2):
        if n_sp > 1:
            with scope("final"):
                absorb(last, half)
        for g in range(heads // 2):
            even, odd = acc[half, 2 * g], acc[half, 2 * g + 1]
            top = jnp.where(lane < hd, pltpu.roll(even, hd, 1), odd)
            low = jnp.where(lane < hd, even, pltpu.roll(odd, hd, 1))
            att[tp, half, :, g * lanes:(g + 1) * lanes] = (top / low).astype(BF16)
        for d in reversed(range(1, n_tp)):
            copy = remote(att.at[tp, half], att.at[tp, half], a_send.at[d, half], a_recv.at[d, half], tp=tp ^ d)
            copy.start()
            waiting.append(copy)

    with scope("gotw2"):
        for d in near:
            for part in turns[d][2:]:
                got_weights(d, part)
    copies["wo"].wait()

    def project(group, half, part):
        return dots(att[group, half], wbuf[group, :, part])

    parts = [slice(t * cols, (t + 1) * cols) for t in range(n_tp)]
    tall = [slice(half * mid, (half + 1) * mid) for half in range(2)]
    with scope("own"):
        for half in range(2):
            for part in parts:
                mixed[tall[half], part] = project(tp, half, part)

    with scope("gotw3"):
        if n_tp == 4:
            for part in range(PARTS):
                got_weights(3, part)
        for d in range(1, n_tp):
            for core in range(1, n_dp):
                source = (dp + n_dp - core) % n_dp
                for part in range(PARTS):
                    ref = wbuf.at[tp ^ d, span(source, part)]
                    remote(ref, ref, f_send.at[d, part, core], f_recv.at[d, part, core], dp=source).wait_recv()
            remote(gate_t.at[tp ^ d], gate_t.at[tp ^ d], gt_send.at[d], gt_recv.at[d], tp=tp ^ d).wait_recv()

    order = [d for d in (2, 3, 1) if d < n_tp]
    for half in range(2):
        for d in order:
            with scope(f"att{half}{d}"):
                ref = att.at[tp ^ d, half]
                remote(ref, ref, a_send.at[d, half], a_recv.at[d, half], tp=tp ^ d).wait_recv()
            if d != order[-1]:
                for part in parts:
                    mixed[tall[half], part] = mixed[tall[half], part] + project(tp ^ d, half, part)
        for t, part in enumerate(parts):
            value = mixed[tall[half], part]
            if order:
                value = value + project(tp ^ order[-1], half, part)
            gate = jnp.concatenate([gate_t[t, j:j + 1, :] for j in range(4)], axis=1)
            out[0, tall[half], part] = (lat[tall[half], part].astype(F32) + gate * value).astype(BF16)

    with scope("sendwait"):
        for copy in waiting:
            copy.wait_send()

        @pl.loop(0, n_sp)
        def _(b):
            for part in range(2):
                @pl.when((b <= sp) & (sp + 1 < n_sp))
                def _():
                    kv_copy(b, sp, 0, part).wait_send()

                @pl.when((b >= sp) & (sp > 0))
                def _():
                    kv_copy(b, sp, 1, part).wait_send()


def on_device(
    sizes, latent, condition, context, context_code, shift_weight, scale_weight, gate_weight,
    norm_gain, query_weight, key_weight, value_weight, output_weight, query_gain, key_gain,
    context_bias,
):
    n_sp, n_tp, n_dp = sizes
    rows, width = latent.shape[1:]
    crows = context.shape[1]
    hd = query_gain.shape[0]
    qcols = query_weight.shape[1]
    heads = qcols // hd
    deep, cols = shift_weight.shape
    vmem = pl.BlockSpec(memory_space=pltpu.VMEM)
    smem = pl.BlockSpec(memory_space=pltpu.SMEM)
    hbm = pl.BlockSpec(memory_space=pl.ANY)
    dma = pltpu.SemaphoreType.DMA
    most = max(rows, crows)
    mid = rows // 2
    lanes = 2 * hd
    scratch = [
        pltpu.VMEM((3, deep, cols), BF16),
        pltpu.VMEM((rows, width), BF16),
        pltpu.VMEM((crows, width), BF16),
        pltpu.VMEM((width, qcols), BF16),
        pltpu.VMEM((lanes, width), BF16),
        pltpu.VMEM((n_tp,) + output_weight.shape, BF16),
        pltpu.VMEM((n_sp, 8, cols // 2), F32),
        pltpu.VMEM((n_tp, 8, cols // 2), F32),
        pltpu.VMEM((n_sp, 4, cols // 4), F32),
        pltpu.VMEM((n_tp, 4, cols // 4), F32),
        pltpu.VMEM((most, width), BF16),
        pltpu.VMEM((n_sp, crows + rows, lanes), BF16),
        pltpu.VMEM((crows + rows, lanes), BF16),
        pltpu.VMEM((2, heads * mid, lanes), BF16),
        pltpu.VMEM((2, heads, mid, lanes), F32),
        pltpu.VMEM((2, heads, mid, lanes), F32),
        pltpu.VMEM((n_tp, 2, mid, qcols), BF16),
        pltpu.VMEM((rows, width), F32),
        pltpu.VMEM((rows, lanes), F32),
        pltpu.VMEM((rows, lanes), F32),
        pltpu.VMEM((rows, 1), F32),
        dma((9,)), pltpu.SemaphoreType.REGULAR,
        dma((n_sp,)), dma((n_sp,)), dma((n_tp,)), dma((n_tp,)),
        dma((n_sp,)), dma((n_sp,)), dma((n_tp,)), dma((n_tp,)),
        dma((2, 2, n_sp)), dma((2, n_sp)),
        dma((n_tp, PARTS)), dma((n_tp, PARTS)), dma((n_tp, PARTS, n_dp)), dma((n_tp, PARTS, n_dp)),
        dma((n_tp, 2)), dma((n_tp, 2)),
    ]
    return pl.pallas_call(
        functools.partial(kernel, sizes),
        out_shape=pltpu.VMEM(latent.shape, BF16),
        in_specs=[vmem] * 5 + [smem] + [hbm] * 9,
        out_specs=vmem,
        scratch_shapes=scratch,
        compiler_params=pltpu.CompilerParams(
            collective_id=0, has_side_effects=True, vmem_limit_bytes=SCOPED_KIB * 1024),
    )(
        condition, context_code, norm_gain[None], query_gain[None], key_gain[None],
        context_bias, latent, context, shift_weight, scale_weight, gate_weight, query_weight,
        key_weight.T, value_weight.T, output_weight,
    )


def solution(mesh):
    sizes = tuple(mesh.shape[axis] for axis in ("sp", "tp", "dp"))
    return jax.shard_map(
        functools.partial(on_device, sizes),
        mesh=mesh,
        in_specs=(
            P("dp", "sp", None),
            P("dp", "sp"),
            P("dp", "sp", None),
            P("sp"),
            P("sp", "tp"),
            P("sp", "tp"),
            P("sp", "tp"),
            P(),
            P(None, "tp"),
            P(None, "tp"),
            P(None, "tp"),
            P("tp", None),
            P(),
            P(),
            P("tp"),
        ),
        out_specs=P("dp", "sp", None),
        check_vma=False,
    )
```

```python
import functools
import math

import jax
import jax.numpy as jnp
from jax import lax
from jax.experimental import pallas as pl
from jax.experimental.pallas import tpu as pltpu
from jax.sharding import PartitionSpec as P

GRID_W = 64
norm_eps = 1e-06
rope_base = 10000.0
F32 = jnp.float32
BF16 = jnp.bfloat16
LANES = 128
LOG2E = math.log2(math.e)
PARTS = 4
GROUP = 2
SCOPED_KIB = 64384


def tables(first, rows, head_dim):
    quarter = head_dim // 4
    half = head_dim // 2
    shape = (rows, 2 * head_dim)
    token = first + lax.broadcasted_iota(jnp.int32, shape, 0)
    lane = lax.broadcasted_iota(jnp.int32, shape, 1) % head_dim
    pair = lane % half
    index = (pair % quarter).astype(F32)
    place = jnp.where(pair < quarter, token // GRID_W, token % GRID_W).astype(F32)
    angle = place * jnp.exp(index * (-math.log(rope_base) / quarter))
    sine = jnp.sin(angle)
    return jnp.cos(angle), jnp.where(lane < half, -sine, sine)


def kernel(
    sizes,
    condition_h, code_h, gain_h, q_gain_h, k_gain_h, bias_h,
    latent, context, shift_w, scale_w, gate_w, wq, wk, wv, wo,
    out,
    condition, code, gain_ref, q_gain, k_gain, bias_ref,
    modw, lat, ctx, wq_v, wkv, wkv_t, wbuf,
    vec_z, vec_t, gate_z, gate_t, normed, kvbuf, vals, q_s, m_s, acc, att, mixed, cos_s, sin_s, inv_s,
    local, met,
    z_send, z_recv, t_send, t_recv, gz_send, gz_recv, gt_send, gt_recv, kv_send, kv_recv,
    w_send, w_recv, f_send, f_recv, a_send, a_recv,
):
    n_sp, n_tp, n_dp = sizes
    sp, tp, dp = lax.axis_index("sp"), lax.axis_index("tp"), lax.axis_index("dp")
    rows, crows = lat.shape[0], ctx.shape[0]
    hd = wk.shape[0]
    qcols = wq_v.shape[1]
    heads = qcols // hd
    width = lat.shape[1]
    cols = width // n_tp
    side = cols // 2
    chip = cols // 4
    mid = rows // 2
    lanes = 2 * hd
    dots = functools.partial(jnp.dot, preferred_element_type=F32)
    dims = (((1,), (1,)), ((), ()))
    scope = jax.named_scope

    barrier = pltpu.get_barrier_semaphore()

    def greet(sem, **where):
        pl.semaphore_signal(sem, inc=1, device_id=where, device_id_type=pl.DeviceIdType.MESH)

    for d in range(1, n_sp):
        greet(barrier, sp=(sp + d) % n_sp)
    for d in range(1, n_tp):
        greet(barrier, tp=tp ^ d)
    for d in range(1, n_dp):
        @pl.when(dp + d < n_dp)
        def _():
            greet(barrier, dp=dp + d)

    copies = {}
    for number, (name, src, dst) in enumerate((
        ("condition", condition_h, condition), ("code", code_h, code),
        ("m0", shift_w, modw.at[0]), ("m1", scale_w, modw.at[1]), ("m2", gate_w, modw.at[2]),
        ("ctx", context.at[0], ctx), ("gain", gain_h, gain_ref), ("wk", wk, wkv.at[:hd]), ("wv", wv, wkv.at[hd:]),
        ("k_gain", k_gain_h, k_gain), ("lat", latent.at[0], lat), ("q_gain", q_gain_h, q_gain), ("bias", bias_h, bias_ref),
        ("wq", wq, wq_v), ("wo", wo, wbuf.at[tp]),
    )):
        copies[name] = pltpu.make_async_copy(src, dst, local.at[number])
        copies[name].start()

    def remote(src, dst, s, r, **where):
        return pltpu.make_async_remote_copy(
            src_ref=src, dst_ref=dst, send_sem=s, recv_sem=r,
            device_id=where, device_id_type=pl.DeviceIdType.MESH)

    with scope("modmat"):
        copies["condition"].wait()
        copies["code"].wait()
        row8 = lax.broadcasted_iota(jnp.int32, (8, condition.shape[1]), 0)
        own_code = condition[...].astype(F32)
        shared_code = code[...].astype(F32)[None]
        both = jnp.where(row8 == 0, own_code, jnp.where(row8 == 1, shared_code, 0.0))
        both = (both / (1.0 + jnp.exp(-both))).astype(BF16)
        pieces = []
        for k in range(2):
            copies[f"m{k}"].wait()
            pieces.append(dots(both, modw[k])[:2])
        rows4 = jnp.concatenate(pieces, axis=0)
        vec_z[sp] = jnp.concatenate([rows4[:, :side], rows4[:, side:]], axis=0)

    with scope("barrier"):
        pl.semaphore_wait(barrier, n_sp + n_tp - 2 + dp)

    z_copies = []
    for d in range(1, n_sp):
        copy = remote(vec_z.at[sp], vec_z.at[sp], z_send.at[d], z_recv.at[d], sp=(sp + d) % n_sp)
        copy.start()
        z_copies.append(copy)
    for d in range(1, n_dp):
        @pl.when(dp - d >= 0)
        def _():
            greet(met, dp=dp - d)

    share = wo.shape[0] // n_dp
    piece = share // PARTS
    near = [d for d in (1, 2) if d < n_tp]
    turns = {1: (2, 3, 0, 1), 2: (0, 1, 2, 3)}
    waiting = []

    def span(core, part):
        return pl.ds(core * share + part * piece, piece)

    def send_weights(turn):
        for d in near:
            part = turns[d][turn]
            copy = remote(wo.at[span(dp, part)], wbuf.at[tp, span(dp, part)],
                          w_send.at[d, part], w_recv.at[d, part], tp=tp ^ d)
            copy.start()
            waiting.append(copy)

    def got_weights(d, part):
        ref = wbuf.at[tp ^ d, span(dp, part)]
        remote(ref, ref, w_send.at[d, part], w_recv.at[d, part], tp=tp ^ d).wait_recv()
        if n_tp == 4 and d < 3 and part in turns[d][:2]:
            copy = remote(ref, ref, w_send.at[3, part], w_recv.at[3, part], tp=tp ^ (3 - d))
            copy.start()
            waiting.append(copy)
        for e in range(1, n_dp):
            copy = remote(ref, ref, f_send.at[d, part, e], f_recv.at[d, part, e], dp=(dp + e) % n_dp)
            copy.start()
            waiting.append(copy)

    send_weights(0)

    with scope("gate"):
        copies["m2"].wait()
        row = dots(both, modw[2])[:1]
        gate_z[sp] = jnp.concatenate([row[:, j * chip:(j + 1) * chip] for j in range(4)], axis=0)
    g_copies = []
    for d in range(1, n_sp):
        copy = remote(gate_z.at[sp], gate_z.at[sp], gz_send.at[d], gz_recv.at[d], sp=(sp + d) % n_sp)
        copy.start()
        g_copies.append(copy)

    with scope("tables"):
        cosine, sine = tables(sp * rows, rows, hd)
        cos_s[...] = cosine
        sin_s[...] = sine
    with scope("inv"):
        copies["ctx"].wait()
        floats = ctx[...].astype(F32)
        inv_c = lax.rsqrt(jnp.mean(floats * floats, axis=-1, keepdims=True) + norm_eps)
        copies["lat"].wait()
        floats = lat[...].astype(F32)
        inv_s[...] = lax.rsqrt(jnp.mean(floats * floats, axis=-1, keepdims=True) + norm_eps)

    with scope("turn"):
        copies["wk"].wait()
        copies["wv"].wait()
        wkv_t[...] = wkv[...].T
    with scope("zwait"):
        for copy in z_copies:
            copy.wait()
    total = vec_z[0]
    for k in range(1, n_sp):
        total = total + vec_z[k]
    vec_t[tp] = total
    for d in reversed(range(1, n_tp)):
        copy = remote(vec_t.at[tp], vec_t.at[tp], t_send.at[d], t_recv.at[d], tp=tp ^ d)
        copy.start()
        waiting.append(copy)
    for turn in range(1, PARTS):
        send_weights(turn)
    with scope("twait"):
        for d in range(1, n_tp):
            remote(vec_t.at[tp ^ d], vec_t.at[tp ^ d], t_send.at[d], t_recv.at[d], tp=tp ^ d).wait_recv()

    def modulate(tokens, inverse, which):
        for t in range(n_tp):
            for k in range(2):
                part = slice(t * cols + k * side, t * cols + (k + 1) * side)
                at = 4 * k + which
                factor = gain_ref[:, part] * (1.0 + vec_t[t, at + 2:at + 3, :])
                shift = vec_t[t, at:at + 1, :]
                normed[:tokens.shape[0], part] = (tokens[:, part].astype(F32) * inverse * factor + shift).astype(BF16)

    def kv_copy(block, target, way, part):
        area = pl.ds(0, crows) if part == 0 else pl.ds(crows, rows)
        ref = kvbuf.at[block, area]
        return remote(ref, ref, kv_send.at[way, part, block], kv_recv.at[part, block], sp=target)

    def send_own(part):
        @pl.when(sp + 1 < n_sp)
        def _():
            kv_copy(sp, sp + 1, 0, part).start()

        @pl.when(sp > 0)
        def _():
            kv_copy(sp, sp - 1, 1, part).start()

    def send_far(part):
        if n_sp > 2:
            @pl.when(sp == 0)
            def _():
                kv_copy(sp, n_sp - 1, 1, part).start()

            @pl.when(sp == n_sp - 1)
            def _():
                kv_copy(sp, 0, 0, part).start()

    def averages(values):
        n = values.shape[1]
        row = lax.broadcasted_iota(jnp.int32, (n, n), 0) // hd
        col = lax.broadcasted_iota(jnp.int32, (n, n), 1) // hd
        spread = jnp.where(row == col, 1.0 / hd, 0.0).astype(BF16)
        return dots((values * values).astype(BF16), spread)

    def swapped(values):
        lane = lax.broadcasted_iota(jnp.int32, values.shape, 1) % hd
        return jnp.where(lane < hd // 2, pltpu.roll(values, lanes - hd // 2, 1), pltpu.roll(values, hd // 2, 1))

    def key_values(count, turn):
        kv = dots(normed[:count], wkv_t[...])
        lane = lax.broadcasted_iota(jnp.int32, kv.shape, 1)
        keys = kv * lax.rsqrt(averages(kv) + norm_eps) * jnp.concatenate([k_gain[...]] * 2, axis=1)
        if turn:
            keys = keys * cos_s[...] + swapped(keys) * sin_s[...]
        return jnp.where(lane < hd, keys, kv).astype(BF16)

    copies["gain"].wait()
    with scope("modctx"):
        modulate(ctx, inv_c, 1)
    with scope("kvctx"):
        copies["k_gain"].wait()
        kvbuf[sp, :crows] = key_values(crows, False)
    send_far(0)
    send_own(0)

    with scope("modlat"):
        modulate(lat, inv_s[...], 0)
    with scope("kvlat"):
        kvbuf[sp, crows:] = key_values(rows, True)
    send_far(1)
    send_own(1)

    with scope("gotw0"):
        for d in range(1, n_dp):
            @pl.when(dp + d < n_dp)
            def _():
                pl.semaphore_wait(met, 1)
        for d in near:
            got_weights(d, turns[d][0])

    with scope("qproj"):
        copies["wq"].wait()
        copies["q_gain"].wait()
        queries = dots(normed[:rows], wq_v[...])
        factor = lax.rsqrt(averages(queries) + norm_eps)
        gains = jnp.concatenate([q_gain[...]] * 2, axis=1) * (hd ** -0.5 * LOG2E)
        lane = lax.broadcasted_iota(jnp.int32, (rows, lanes), 1)
        for g in range(heads // 2):
            pair = slice(g * lanes, (g + 1) * lanes)
            two = queries[:, pair] * factor[:, pair] * gains
            two = two * cos_s[...] + swapped(two) * sin_s[...]
            for h, one in ((2 * g, two), (2 * g + 1, pltpu.roll(two, hd, 1))):
                one = jnp.where(lane < hd, one, 0.0).astype(BF16)
                for half in range(2):
                    q_s[half, h * mid:(h + 1) * mid] = one[half * mid:(half + 1) * mid]

    with scope("gatez"):
        for copy in g_copies:
            copy.wait()
        total = gate_z[0]
        for k in range(1, n_sp):
            total = total + gate_z[k]
        gate_t[tp] = total
    for d in range(1, n_tp):
        copy = remote(gate_t.at[tp], gate_t.at[tp], gt_send.at[d], gt_recv.at[d], tp=tp ^ d)
        copy.start()
        waiting.append(copy)

    def spread(column, count):
        if count % LANES == 0:
            return jnp.concatenate([column] * (count // LANES), axis=1)
        return column[:, :count]

    def prepare(block):
        pairs = kvbuf[block]
        lane = lax.broadcasted_iota(jnp.int32, pairs.shape, 1)
        vals[...] = jnp.where(lane < hd, jnp.ones_like(pairs), pairs)

    def absorb(block, half, first=False):
        def scores(g):
            query = q_s[half, g * GROUP * mid:(g + 1) * GROUP * mid]
            return (lax.dot_general(query, kvbuf[block, :crows], dims, preferred_element_type=F32),
                    lax.dot_general(query, kvbuf[block, crows:], dims, preferred_element_type=F32))

        ahead = scores(0)
        for g in range(heads // GROUP):
            all_c, all_l = ahead
            if (g + 1) * GROUP < heads:
                ahead = scores(g + 1)
            shares, weights_c, weights_l = [], [], []
            for k in range(GROUP):
                h = g * GROUP + k
                s_c, s_l = all_c[k * mid:(k + 1) * mid], all_l[k * mid:(k + 1) * mid]
                bias = bias_ref[h] * LOG2E
                top = jnp.maximum(s_c.max(axis=1, keepdims=True) + bias, s_l.max(axis=1, keepdims=True))
                top = jnp.broadcast_to(top, (mid, lanes))
                new = top if first else jnp.maximum(m_s[half, h], top)
                weights_c.append(jnp.exp2(s_c - spread(new - bias, crows)).astype(BF16))
                weights_l.append(jnp.exp2(s_l - spread(new, rows)).astype(BF16))
                shares.append(None if first else jnp.exp2(m_s[half, h] - new))
                m_s[half, h] = new
            more = (dots(jnp.concatenate(weights_c, axis=0), vals[:crows])
                    + dots(jnp.concatenate(weights_l, axis=0), vals[crows:]))
            for k in range(GROUP):
                h = g * GROUP + k
                own = more[k * mid:(k + 1) * mid]
                acc[half, h] = own if first else acc[half, h] * shares[k] + own

    def absorb_all(block, first=False):
        prepare(block)

        @pl.loop(0, 2)
        def _(half):
            absorb(block, half, first)

    lower = 2 * sp < n_sp
    edge = (sp == 0) | (sp == n_sp - 1)

    def away(s):
        if n_sp < 3:
            return s
        return jnp.where(edge & (s > 1), jnp.where(s == 2, n_sp - 1, s - 1), s)

    reach = jnp.where(edge, away(n_sp - 1), jnp.where(lower, n_sp - 1 - sp, sp))
    last = jnp.where(lower, sp + reach, sp - reach)

    def passes(block, target):
        if n_sp < 3:
            return (target >= 0) & (target < n_sp)
        far = ((block == 0) & (target == n_sp - 1)) | ((block == n_sp - 1) & (target == 0))
        return (target >= 0) & (target < n_sp) & jnp.logical_not(far)

    def forward(s, parts=(0, 1)):
        d = away(s)
        for part in parts:
            @pl.when(sp - d >= 0)
            def _():
                kv_copy(sp - d, sp, 0, part).wait_recv()

                @pl.when(passes(sp - d, sp + 1))
                def _():
                    kv_copy(sp - d, sp + 1, 0, part).start()

            @pl.when(sp + d < n_sp)
            def _():
                kv_copy(sp + d, sp, 1, part).wait_recv()

                @pl.when(passes(sp + d, sp - 1))
                def _():
                    kv_copy(sp + d, sp - 1, 1, part).start()

    copies["bias"].wait()
    with scope("absorb0"):
        prepare(sp)
        absorb(sp, 0, True)
    if n_sp > 1:
        with scope("fwd1c"):
            forward(1, (0,))
    with scope("absorb0"):
        absorb(sp, 1, True)
    if n_sp > 1:
        with scope("fwd1l"):
            forward(1, (1,))
    with scope("gotw1"):
        for d in near:
            got_weights(d, turns[d][1])

    def side_block(s, long):
        block = jnp.where(lower == long, sp + away(s), sp - away(s))

        @pl.when((block >= 0) & (block < n_sp) & (block != last))
        def _():
            with scope("absorb"):
                absorb_all(block)

    @pl.loop(1, n_sp)
    def _(s):
        side_block(s, True)

        @pl.when(s + 1 < n_sp)
        def _():
            with scope("fwd"):
                forward(s + 1)
        side_block(s, False)

    if n_sp > 1:
        with scope("prepare"):
            prepare(last)
    lane = lax.broadcasted_iota(jnp.int32, (mid, lanes), 1)
    for half in range(2):
        if n_sp > 1:
            with scope("final"):
                absorb(last, half)
        for g in range(heads // 2):
            even, odd = acc[half, 2 * g], acc[half, 2 * g + 1]
            top = jnp.where(lane < hd, pltpu.roll(even, hd, 1), odd)
            low = jnp.where(lane < hd, even, pltpu.roll(odd, hd, 1))
            att[tp, half, :, g * lanes:(g + 1) * lanes] = (top / low).astype(BF16)
        for d in reversed(range(1, n_tp)):
            copy = remote(att.at[tp, half], att.at[tp, half], a_send.at[d, half], a_recv.at[d, half], tp=tp ^ d)
            copy.start()
            waiting.append(copy)

    with scope("gotw2"):
        for d in near:
            for part in turns[d][2:]:
                got_weights(d, part)
    copies["wo"].wait()

    def project(group, half, part):
        return dots(att[group, half], wbuf[group, :, part])

    parts = [slice(t * cols, (t + 1) * cols) for t in range(n_tp)]
    tall = [slice(half * mid, (half + 1) * mid) for half in range(2)]
    with scope("own"):
        for half in range(2):
            for part in parts:
                mixed[tall[half], part] = project(tp, half, part)

    with scope("gotw3"):
        if n_tp == 4:
            for part in range(PARTS):
                got_weights(3, part)
        for d in range(1, n_tp):
            for core in range(1, n_dp):
                source = (dp + n_dp - core) % n_dp
                for part in range(PARTS):
                    ref = wbuf.at[tp ^ d, span(source, part)]
                    remote(ref, ref, f_send.at[d, part, core], f_recv.at[d, part, core], dp=source).wait_recv()
            remote(gate_t.at[tp ^ d], gate_t.at[tp ^ d], gt_send.at[d], gt_recv.at[d], tp=tp ^ d).wait_recv()

    order = [d for d in (2, 3, 1) if d < n_tp]
    for half in range(2):
        for d in order:
            with scope(f"att{half}{d}"):
                ref = att.at[tp ^ d, half]
                remote(ref, ref, a_send.at[d, half], a_recv.at[d, half], tp=tp ^ d).wait_recv()
            if d != order[-1]:
                for part in parts:
                    mixed[tall[half], part] = mixed[tall[half], part] + project(tp ^ d, half, part)
        for t, part in enumerate(parts):
            value = mixed[tall[half], part]
            if order:
                value = value + project(tp ^ order[-1], half, part)
            gate = jnp.concatenate([gate_t[t, j:j + 1, :] for j in range(4)], axis=1)
            out[0, tall[half], part] = (lat[tall[half], part].astype(F32) + gate * value).astype(BF16)

    with scope("sendwait"):
        for copy in waiting:
            copy.wait_send()

        @pl.loop(0, n_sp)
        def _(b):
            for part in range(2):
                @pl.when((b <= sp) & passes(b, sp + 1) | (b == sp) & (sp == n_sp - 1) & (n_sp > 2))
                def _():
                    kv_copy(b, sp, 0, part).wait_send()

                @pl.when((b >= sp) & passes(b, sp - 1) | (b == sp) & (sp == 0) & (n_sp > 2))
                def _():
                    kv_copy(b, sp, 1, part).wait_send()


def on_device(
    sizes, latent, condition, context, context_code, shift_weight, scale_weight, gate_weight,
    norm_gain, query_weight, key_weight, value_weight, output_weight, query_gain, key_gain,
    context_bias,
):
    n_sp, n_tp, n_dp = sizes
    rows, width = latent.shape[1:]
    crows = context.shape[1]
    hd = query_gain.shape[0]
    qcols = query_weight.shape[1]
    heads = qcols // hd
    deep, cols = shift_weight.shape
    vmem = pl.BlockSpec(memory_space=pltpu.VMEM)
    hbm = pl.BlockSpec(memory_space=pl.ANY)
    dma = pltpu.SemaphoreType.DMA
    most = max(rows, crows)
    mid = rows // 2
    lanes = 2 * hd
    scratch = [
        pltpu.VMEM((1, deep), BF16), pltpu.VMEM((deep,), BF16), pltpu.VMEM((1, width), F32),
        pltpu.VMEM((1, hd), F32), pltpu.VMEM((1, hd), F32), pltpu.SMEM((heads,), F32),
        pltpu.VMEM((3, deep, cols), BF16),
        pltpu.VMEM((rows, width), BF16),
        pltpu.VMEM((crows, width), BF16),
        pltpu.VMEM((width, qcols), BF16),
        pltpu.VMEM((lanes, width), BF16),
        pltpu.VMEM((width, lanes), BF16),
        pltpu.VMEM((n_tp,) + output_weight.shape, BF16),
        pltpu.VMEM((n_sp, 8, cols // 2), F32),
        pltpu.VMEM((n_tp, 8, cols // 2), F32),
        pltpu.VMEM((n_sp, 4, cols // 4), F32),
        pltpu.VMEM((n_tp, 4, cols // 4), F32),
        pltpu.VMEM((most, width), BF16),
        pltpu.VMEM((n_sp, crows + rows, lanes), BF16),
        pltpu.VMEM((crows + rows, lanes), BF16),
        pltpu.VMEM((2, heads * mid, lanes), BF16),
        pltpu.VMEM((2, heads, mid, lanes), F32),
        pltpu.VMEM((2, heads, mid, lanes), F32),
        pltpu.VMEM((n_tp, 2, mid, qcols), BF16),
        pltpu.VMEM((rows, width), F32),
        pltpu.VMEM((rows, lanes), F32),
        pltpu.VMEM((rows, lanes), F32),
        pltpu.VMEM((rows, 1), F32),
        dma((15,)), pltpu.SemaphoreType.REGULAR,
        dma((n_sp,)), dma((n_sp,)), dma((n_tp,)), dma((n_tp,)),
        dma((n_sp,)), dma((n_sp,)), dma((n_tp,)), dma((n_tp,)),
        dma((2, 2, n_sp)), dma((2, n_sp)),
        dma((n_tp, PARTS)), dma((n_tp, PARTS)), dma((n_tp, PARTS, n_dp)), dma((n_tp, PARTS, n_dp)),
        dma((n_tp, 2)), dma((n_tp, 2)),
    ]
    return pl.pallas_call(
        functools.partial(kernel, sizes),
        out_shape=pltpu.VMEM(latent.shape, BF16),
        in_specs=[hbm] * 15,
        out_specs=vmem,
        scratch_shapes=scratch,
        compiler_params=pltpu.CompilerParams(
            collective_id=0, has_side_effects=True, vmem_limit_bytes=SCOPED_KIB * 1024),
    )(
        condition, context_code, norm_gain[None], query_gain[None], key_gain[None],
        context_bias, latent, context, shift_weight, scale_weight, gate_weight, query_weight,
        key_weight.T, value_weight.T, output_weight,
    )


def solution(mesh):
    sizes = tuple(mesh.shape[axis] for axis in ("sp", "tp", "dp"))
    return jax.shard_map(
        functools.partial(on_device, sizes),
        mesh=mesh,
        in_specs=(
            P("dp", "sp", None),
            P("dp", "sp"),
            P("dp", "sp", None),
            P("sp"),
            P("sp", "tp"),
            P("sp", "tp"),
            P("sp", "tp"),
            P(),
            P(None, "tp"),
            P(None, "tp"),
            P(None, "tp"),
            P("tp", None),
            P(),
            P(),
            P("tp"),
        ),
        out_specs=P("dp", "sp", None),
        check_vma=False,
    )
```

```python
import functools
import math

import jax
import jax.numpy as jnp
from jax import lax
from jax.experimental import pallas as pl
from jax.experimental.pallas import tpu as pltpu
from jax.sharding import PartitionSpec as P

GRID_W = 64
norm_eps = 1e-06
rope_base = 10000.0
F32 = jnp.float32
BF16 = jnp.bfloat16
LANES = 128
LOG2E = math.log2(math.e)
PARTS = 4
GROUP = 2
SCOPED_KIB = 64384


def tables(first, rows, head_dim):
    quarter = head_dim // 4
    half = head_dim // 2
    shape = (rows, 2 * head_dim)
    token = first + lax.broadcasted_iota(jnp.int32, shape, 0)
    lane = lax.broadcasted_iota(jnp.int32, shape, 1) % head_dim
    pair = lane % half
    index = (pair % quarter).astype(F32)
    place = jnp.where(pair < quarter, token // GRID_W, token % GRID_W).astype(F32)
    angle = place * jnp.exp(index * (-math.log(rope_base) / quarter))
    sine = jnp.sin(angle)
    return jnp.cos(angle), jnp.where(lane < half, -sine, sine)


def kernel(
    sizes,
    condition_h, code_h, gain_h, q_gain_h, k_gain_h, bias_h,
    latent, context, shift_w, scale_w, gate_w, wq, wk, wv, wo,
    out,
    condition, code, gain_ref, q_gain, k_gain, bias_ref,
    modw, lat, ctx, wq_v, wkv, wkv_t, wbuf,
    vec_z, vec_t, gate_z, gate_t, normed, kvbuf, vals, q_s, m_s, acc, att, mixed, cos_s, sin_s, inv_s,
    local, met, sent, came, kv_send, kv_recv, w_recv, x_recv, f_recv, a_recv,
):
    n_sp, n_tp, n_dp = sizes
    sp, tp, dp = lax.axis_index("sp"), lax.axis_index("tp"), lax.axis_index("dp")
    rows, crows = lat.shape[0], ctx.shape[0]
    hd = wk.shape[0]
    qcols = wq_v.shape[1]
    heads = qcols // hd
    width = lat.shape[1]
    cols = width // n_tp
    side = cols // 2
    chip = cols // 4
    mid = rows // 2
    lanes = 2 * hd
    dots = functools.partial(jnp.dot, preferred_element_type=F32)
    dims = (((1,), (1,)), ((), ()))
    scope = jax.named_scope

    barrier = pltpu.get_barrier_semaphore()

    def greet(sem, **where):
        pl.semaphore_signal(sem, inc=1, device_id=where, device_id_type=pl.DeviceIdType.MESH)

    for d in range(1, n_sp):
        greet(barrier, sp=(sp + d) % n_sp)
    for d in range(1, n_tp):
        greet(barrier, tp=tp ^ d)
    for d in range(1, n_dp):
        @pl.when(dp + d < n_dp)
        def _():
            greet(barrier, dp=dp + d)

    copies = {}

    def load(number, name, src, dst):
        copies[name] = pltpu.make_async_copy(src, dst, local.at[number])
        copies[name].start()

    load(0, "condition", condition_h, condition)
    load(1, "code", code_h, code)
    load(2, "m0", shift_w, modw.at[0])
    load(3, "m1", scale_w, modw.at[1])
    load(4, "m2", gate_w, modw.at[2])
    load(5, "ctx", context.at[0], ctx)
    load(6, "gain", gain_h, gain_ref)
    load(7, "wk", wk, wkv.at[:hd])
    load(7, "wv", wv, wkv.at[hd:])
    load(8, "lat", latent.at[0], lat)
    load(9, "k_gain", k_gain_h, k_gain)

    def drain(ref, sem):
        pltpu.make_async_copy(ref, ref, sem).wait()

    def remote(src, dst, s, r, **where):
        return pltpu.make_async_remote_copy(
            src_ref=src, dst_ref=dst, send_sem=s, recv_sem=r,
            device_id=where, device_id_type=pl.DeviceIdType.MESH)

    with scope("modmat"):
        copies["condition"].wait()
        copies["code"].wait()
        row8 = lax.broadcasted_iota(jnp.int32, (8, condition.shape[1]), 0)
        own_code = condition[...].astype(F32)
        shared_code = code[...].astype(F32)[None]
        both = jnp.where(row8 == 0, own_code, jnp.where(row8 == 1, shared_code, 0.0))
        both = (both / (1.0 + jnp.exp(-both))).astype(BF16)
        pieces = []
        for k in range(2):
            copies[f"m{k}"].wait()
            pieces.append(dots(both, modw[k])[:2])
        rows4 = jnp.concatenate(pieces, axis=0)
        vec_z[sp] = jnp.concatenate([rows4[:, :side], rows4[:, side:]], axis=0)

    load(0, "q_gain", q_gain_h, q_gain)
    load(1, "bias", bias_h, bias_ref)
    load(2, "wq", wq, wq_v)
    load(3, "wo", wo, wbuf.at[tp])

    with scope("barrier"):
        pl.semaphore_wait(barrier, n_sp + n_tp - 2 + dp)

    for d in range(1, n_sp):
        remote(vec_z.at[sp], vec_z.at[sp], sent.at[0], came.at[0], sp=(sp + d) % n_sp).start()
    for d in range(1, n_dp):
        @pl.when(dp - d >= 0)
        def _():
            greet(met, dp=dp - d)

    share = wo.shape[0] // n_dp
    piece = share // PARTS
    near = [d for d in (1, 2) if d < n_tp]
    turns = {1: ((2, 1), (3, 1), (0, 2)), 2: ((0, 1), (1, 1), (2, 2))}

    def span(core, first, count):
        return pl.ds(core * share + first * piece, count * piece)

    def send_weights(turn):
        for d in near:
            area = span(dp, *turns[d][turn])
            remote(wo.at[area], wbuf.at[tp, area], sent.at[4], w_recv.at[d - 1, turn], tp=tp ^ d).start()

    def share_weights(ref):
        for e in range(1, n_dp):
            remote(ref, ref, sent.at[5], f_recv.at[e - 1], dp=(dp + e) % n_dp).start()

    def got_weights(d, turn):
        ref = wbuf.at[tp ^ d, span(dp, *turns[d][turn])]
        drain(ref, w_recv.at[d - 1, turn])
        if n_tp == 4 and turn < 2:
            remote(ref, ref, sent.at[4], x_recv.at[d - 1], tp=tp ^ (3 - d)).start()
        share_weights(ref)

    def got_far():
        for d in near:
            ref = wbuf.at[tp ^ 3, span(dp, turns[d][0][0], 2)]
            drain(ref, x_recv.at[d - 1])
            share_weights(ref)

    send_weights(0)

    with scope("gate"):
        copies["m2"].wait()
        row = dots(both, modw[2])[:1]
        gate_z[sp] = jnp.concatenate([row[:, j * chip:(j + 1) * chip] for j in range(4)], axis=0)
    for d in range(1, n_sp):
        remote(gate_z.at[sp], gate_z.at[sp], sent.at[2], came.at[2], sp=(sp + d) % n_sp).start()

    with scope("tables"):
        cosine, sine = tables(sp * rows, rows, hd)
        cos_s[...] = cosine
        sin_s[...] = sine
    with scope("inv"):
        copies["ctx"].wait()
        floats = ctx[...].astype(F32)
        inv_c = lax.rsqrt(jnp.mean(floats * floats, axis=-1, keepdims=True) + norm_eps)
        copies["lat"].wait()
        floats = lat[...].astype(F32)
        inv_s[...] = lax.rsqrt(jnp.mean(floats * floats, axis=-1, keepdims=True) + norm_eps)

    with scope("turn"):
        drain(wkv, local.at[7])
        wkv_t[...] = wkv[...].T
    with scope("zwait"):
        if n_sp > 1:
            drain(vec_z.at[:n_sp - 1], came.at[0])
    total = vec_z[0]
    for k in range(1, n_sp):
        total = total + vec_z[k]
    vec_t[tp] = total
    for d in reversed(range(1, n_tp)):
        remote(vec_t.at[tp], vec_t.at[tp], sent.at[1], came.at[1], tp=tp ^ d).start()
    for turn in (1, 2):
        send_weights(turn)
    with scope("twait"):
        if n_tp > 1:
            drain(vec_t.at[:n_tp - 1], came.at[1])

    def modulate(tokens, inverse, which):
        for t in range(n_tp):
            for k in range(2):
                part = slice(t * cols + k * side, t * cols + (k + 1) * side)
                at = 4 * k + which
                factor = gain_ref[:, part] * (1.0 + vec_t[t, at + 2:at + 3, :])
                shift = vec_t[t, at:at + 1, :]
                normed[:tokens.shape[0], part] = (tokens[:, part].astype(F32) * inverse * factor + shift).astype(BF16)

    def kv_copy(block, target, way, part):
        area = pl.ds(0, crows) if part == 0 else pl.ds(crows, rows)
        ref = kvbuf.at[block, area]
        return remote(ref, ref, kv_send.at[way, block], kv_recv.at[part, block], sp=target)

    def send_own(part):
        @pl.when(sp + 1 < n_sp)
        def _():
            kv_copy(sp, sp + 1, 0, part).start()

        @pl.when(sp > 0)
        def _():
            kv_copy(sp, sp - 1, 1, part).start()

    def send_far(part):
        if n_sp > 2:
            @pl.when(sp == 0)
            def _():
                kv_copy(sp, n_sp - 1, 1, part).start()

            @pl.when(sp == n_sp - 1)
            def _():
                kv_copy(sp, 0, 0, part).start()

    def averages(values):
        n = values.shape[1]
        row = lax.broadcasted_iota(jnp.int32, (n, n), 0) // hd
        col = lax.broadcasted_iota(jnp.int32, (n, n), 1) // hd
        spread = jnp.where(row == col, 1.0 / hd, 0.0).astype(BF16)
        return dots((values * values).astype(BF16), spread)

    def swapped(values):
        lane = lax.broadcasted_iota(jnp.int32, values.shape, 1) % hd
        return jnp.where(lane < hd // 2, pltpu.roll(values, lanes - hd // 2, 1), pltpu.roll(values, hd // 2, 1))

    def key_values(count, turn):
        kv = dots(normed[:count], wkv_t[...])
        lane = lax.broadcasted_iota(jnp.int32, kv.shape, 1)
        keys = kv * lax.rsqrt(averages(kv) + norm_eps) * jnp.concatenate([k_gain[...]] * 2, axis=1)
        if turn:
            keys = keys * cos_s[...] + swapped(keys) * sin_s[...]
        return jnp.where(lane < hd, keys, kv).astype(BF16)

    copies["gain"].wait()
    with scope("modctx"):
        modulate(ctx, inv_c, 1)
    with scope("kvctx"):
        copies["k_gain"].wait()
        kvbuf[sp, :crows] = key_values(crows, False)
    send_far(0)
    send_own(0)

    with scope("modlat"):
        modulate(lat, inv_s[...], 0)
    with scope("kvlat"):
        kvbuf[sp, crows:] = key_values(rows, True)
    send_far(1)
    send_own(1)

    with scope("gotw0"):
        for d in range(1, n_dp):
            @pl.when(dp + d < n_dp)
            def _():
                pl.semaphore_wait(met, 1)
        for d in near:
            got_weights(d, 0)

    with scope("qproj"):
        copies["wq"].wait()
        copies["q_gain"].wait()
        queries = dots(normed[:rows], wq_v[...])
        factor = lax.rsqrt(averages(queries) + norm_eps)
        gains = jnp.concatenate([q_gain[...]] * 2, axis=1) * (hd ** -0.5 * LOG2E)
        lane = lax.broadcasted_iota(jnp.int32, (rows, lanes), 1)
        for g in range(heads // 2):
            pair = slice(g * lanes, (g + 1) * lanes)
            two = queries[:, pair] * factor[:, pair] * gains
            two = two * cos_s[...] + swapped(two) * sin_s[...]
            for h, one in ((2 * g, two), (2 * g + 1, pltpu.roll(two, hd, 1))):
                one = jnp.where(lane < hd, one, 0.0).astype(BF16)
                for half in range(2):
                    q_s[half, h * mid:(h + 1) * mid] = one[half * mid:(half + 1) * mid]

    with scope("gatez"):
        if n_sp > 1:
            drain(gate_z.at[:n_sp - 1], came.at[2])
        total = gate_z[0]
        for k in range(1, n_sp):
            total = total + gate_z[k]
        gate_t[tp] = total
    for d in range(1, n_tp):
        remote(gate_t.at[tp], gate_t.at[tp], sent.at[3], came.at[3], tp=tp ^ d).start()

    def spread(column, count):
        if count % LANES == 0:
            return jnp.concatenate([column] * (count // LANES), axis=1)
        return column[:, :count]

    def prepare(block):
        pairs = kvbuf[block]
        lane = lax.broadcasted_iota(jnp.int32, pairs.shape, 1)
        vals[...] = jnp.where(lane < hd, jnp.ones_like(pairs), pairs)

    def absorb(block, half, first=False):
        def scores(g):
            query = q_s[half, g * GROUP * mid:(g + 1) * GROUP * mid]
            return (lax.dot_general(query, kvbuf[block, :crows], dims, preferred_element_type=F32),
                    lax.dot_general(query, kvbuf[block, crows:], dims, preferred_element_type=F32))

        ahead = scores(0)
        for g in range(heads // GROUP):
            all_c, all_l = ahead
            if (g + 1) * GROUP < heads:
                ahead = scores(g + 1)
            shares, weights_c, weights_l = [], [], []
            for k in range(GROUP):
                h = g * GROUP + k
                s_c, s_l = all_c[k * mid:(k + 1) * mid], all_l[k * mid:(k + 1) * mid]
                bias = bias_ref[h] * LOG2E
                top = jnp.maximum(s_c.max(axis=1, keepdims=True) + bias, s_l.max(axis=1, keepdims=True))
                top = jnp.broadcast_to(top, (mid, lanes))
                new = top if first else jnp.maximum(m_s[half, h], top)
                weights_c.append(jnp.exp2(s_c - spread(new - bias, crows)).astype(BF16))
                weights_l.append(jnp.exp2(s_l - spread(new, rows)).astype(BF16))
                shares.append(None if first else jnp.exp2(m_s[half, h] - new))
                m_s[half, h] = new
            more = (dots(jnp.concatenate(weights_c, axis=0), vals[:crows])
                    + dots(jnp.concatenate(weights_l, axis=0), vals[crows:]))
            for k in range(GROUP):
                h = g * GROUP + k
                own = more[k * mid:(k + 1) * mid]
                acc[half, h] = own if first else acc[half, h] * shares[k] + own

    def absorb_all(block, first=False):
        prepare(block)

        @pl.loop(0, 2)
        def _(half):
            absorb(block, half, first)

    lower = 2 * sp < n_sp
    edge = (sp == 0) | (sp == n_sp - 1)

    def away(s):
        if n_sp < 3:
            return s
        return jnp.where(edge & (s > 1), jnp.where(s == 2, n_sp - 1, s - 1), s)

    reach = jnp.where(edge, away(n_sp - 1), jnp.where(lower, n_sp - 1 - sp, sp))
    last = jnp.where(lower, sp + reach, sp - reach)

    def passes(block, target):
        if n_sp < 3:
            return (target >= 0) & (target < n_sp)
        far = ((block == 0) & (target == n_sp - 1)) | ((block == n_sp - 1) & (target == 0))
        return (target >= 0) & (target < n_sp) & jnp.logical_not(far)

    def forward(s, parts=(0, 1)):
        d = away(s)
        for part in parts:
            @pl.when(sp - d >= 0)
            def _():
                kv_copy(sp - d, sp, 0, part).wait_recv()

                @pl.when(passes(sp - d, sp + 1))
                def _():
                    kv_copy(sp - d, sp + 1, 0, part).start()

            @pl.when(sp + d < n_sp)
            def _():
                kv_copy(sp + d, sp, 1, part).wait_recv()

                @pl.when(passes(sp + d, sp - 1))
                def _():
                    kv_copy(sp + d, sp - 1, 1, part).start()

    copies["bias"].wait()
    with scope("absorb0"):
        prepare(sp)
        absorb(sp, 0, True)
    if n_sp > 1:
        with scope("fwd1c"):
            forward(1, (0,))
    with scope("absorb0"):
        absorb(sp, 1, True)
    if n_sp > 1:
        with scope("fwd1l"):
            forward(1, (1,))
    with scope("gotw1"):
        for d in near:
            got_weights(d, 1)

    def side_block(s, long):
        block = jnp.where(lower == long, sp + away(s), sp - away(s))

        @pl.when((block >= 0) & (block < n_sp) & (block != last))
        def _():
            with scope("absorb"):
                absorb_all(block)

    @pl.loop(1, n_sp)
    def _(s):
        side_block(s, True)

        @pl.when(s + 1 < n_sp)
        def _():
            with scope("fwd"):
                forward(s + 1)
        side_block(s, False)

    with scope("gotw2"):
        for d in near:
            got_weights(d, 2)
    if n_sp > 1:
        with scope("prepare"):
            prepare(last)
    lane = lax.broadcasted_iota(jnp.int32, (mid, lanes), 1)
    for half in range(2):
        if n_sp > 1:
            with scope("final"):
                absorb(last, half)
        for g in range(heads // 2):
            even, odd = acc[half, 2 * g], acc[half, 2 * g + 1]
            top = jnp.where(lane < hd, pltpu.roll(even, hd, 1), odd)
            low = jnp.where(lane < hd, even, pltpu.roll(odd, hd, 1))
            att[tp, half, :, g * lanes:(g + 1) * lanes] = (top / low).astype(BF16)
        for d in reversed(range(1, n_tp)):
            remote(att.at[tp, half], att.at[tp, half], sent.at[6], a_recv.at[half * d], tp=tp ^ d).start()

    copies["wo"].wait()

    def project(group, half, part):
        return dots(att[group, half], wbuf[group, :, part])

    parts = [slice(t * cols, (t + 1) * cols) for t in range(n_tp)]
    tall = [slice(half * mid, (half + 1) * mid) for half in range(2)]
    with scope("own"):
        for half in range(2):
            for part in parts:
                mixed[tall[half], part] = project(tp, half, part)

    with scope("gotw3"):
        if n_tp == 4:
            got_far()
        for e in range(1, n_dp):
            if n_tp > 1:
                drain(wbuf.at[:n_tp - 1, :share], f_recv.at[e - 1])
        if n_tp > 1:
            drain(gate_t.at[:n_tp - 1], came.at[3])

    order = [d for d in (2, 3, 1) if d < n_tp]
    for half in range(2):
        for d in order:
            with scope(f"att{half}{d}"):
                if half == 0 and d == order[0]:
                    drain(att.at[:n_tp - 1, 0], a_recv.at[0])
                if half == 1:
                    drain(att.at[tp ^ d, 1], a_recv.at[d])
            if d != order[-1]:
                for part in parts:
                    mixed[tall[half], part] = mixed[tall[half], part] + project(tp ^ d, half, part)
        for t, part in enumerate(parts):
            value = mixed[tall[half], part]
            if order:
                value = value + project(tp ^ order[-1], half, part)
            gate = jnp.concatenate([gate_t[t, j:j + 1, :] for j in range(4)], axis=1)
            out[0, tall[half], part] = (lat[tall[half], part].astype(F32) + gate * value).astype(BF16)

    with scope("sendwait"):
        if n_sp > 1:
            drain(vec_z.at[:n_sp - 1], sent.at[0])
            drain(gate_z.at[:n_sp - 1], sent.at[2])
        if n_tp > 1:
            drain(vec_t.at[:n_tp - 1], sent.at[1])
            drain(gate_t.at[:n_tp - 1], sent.at[3])
            drain(wbuf.at[:n_tp - 1, :share], sent.at[4])
            for e in range(1, n_dp):
                drain(wbuf.at[:n_tp - 1, :share], sent.at[5])
            drain(att.at[:n_tp - 1], sent.at[6])

        @pl.loop(0, n_sp)
        def _(b):
            @pl.when((b <= sp) & passes(b, sp + 1) | (b == sp) & (sp == n_sp - 1) & (n_sp > 2))
            def _():
                drain(kvbuf.at[b], kv_send.at[0, b])

            @pl.when((b >= sp) & passes(b, sp - 1) | (b == sp) & (sp == 0) & (n_sp > 2))
            def _():
                drain(kvbuf.at[b], kv_send.at[1, b])


def on_device(
    sizes, latent, condition, context, context_code, shift_weight, scale_weight, gate_weight,
    norm_gain, query_weight, key_weight, value_weight, output_weight, query_gain, key_gain,
    context_bias,
):
    n_sp, n_tp, n_dp = sizes
    rows, width = latent.shape[1:]
    crows = context.shape[1]
    hd = query_gain.shape[0]
    qcols = query_weight.shape[1]
    heads = qcols // hd
    deep, cols = shift_weight.shape
    vmem = pl.BlockSpec(memory_space=pltpu.VMEM)
    hbm = pl.BlockSpec(memory_space=pl.ANY)
    dma = pltpu.SemaphoreType.DMA
    most = max(rows, crows)
    mid = rows // 2
    lanes = 2 * hd
    scratch = [
        pltpu.VMEM((1, deep), BF16), pltpu.VMEM((deep,), BF16), pltpu.VMEM((1, width), F32),
        pltpu.VMEM((1, hd), F32), pltpu.VMEM((1, hd), F32), pltpu.SMEM((heads,), F32),
        pltpu.VMEM((3, deep, cols), BF16),
        pltpu.VMEM((rows, width), BF16),
        pltpu.VMEM((crows, width), BF16),
        pltpu.VMEM((width, qcols), BF16),
        pltpu.VMEM((lanes, width), BF16),
        pltpu.VMEM((width, lanes), BF16),
        pltpu.VMEM((n_tp,) + output_weight.shape, BF16),
        pltpu.VMEM((n_sp, 8, cols // 2), F32),
        pltpu.VMEM((n_tp, 8, cols // 2), F32),
        pltpu.VMEM((n_sp, 4, cols // 4), F32),
        pltpu.VMEM((n_tp, 4, cols // 4), F32),
        pltpu.VMEM((most, width), BF16),
        pltpu.VMEM((n_sp, crows + rows, lanes), BF16),
        pltpu.VMEM((crows + rows, lanes), BF16),
        pltpu.VMEM((2, heads * mid, lanes), BF16),
        pltpu.VMEM((2, heads, mid, lanes), F32),
        pltpu.VMEM((2, heads, mid, lanes), F32),
        pltpu.VMEM((n_tp, 2, mid, qcols), BF16),
        pltpu.VMEM((rows, width), F32),
        pltpu.VMEM((rows, lanes), F32),
        pltpu.VMEM((rows, lanes), F32),
        pltpu.VMEM((rows, 1), F32),
        dma((10,)), pltpu.SemaphoreType.REGULAR, dma((7,)), dma((4,)),
        dma((2, n_sp)), dma((2, n_sp)), dma((2, 3)), dma((2,)), dma((n_dp,)), dma((n_tp,)),
    ]
    return pl.pallas_call(
        functools.partial(kernel, sizes),
        out_shape=pltpu.VMEM(latent.shape, BF16),
        in_specs=[hbm] * 15,
        out_specs=vmem,
        scratch_shapes=scratch,
        compiler_params=pltpu.CompilerParams(
            collective_id=0, has_side_effects=True, vmem_limit_bytes=SCOPED_KIB * 1024),
    )(
        condition, context_code, norm_gain[None], query_gain[None], key_gain[None],
        context_bias, latent, context, shift_weight, scale_weight, gate_weight, query_weight,
        key_weight.T, value_weight.T, output_weight,
    )


def solution(mesh):
    sizes = tuple(mesh.shape[axis] for axis in ("sp", "tp", "dp"))
    return jax.shard_map(
        functools.partial(on_device, sizes),
        mesh=mesh,
        in_specs=(
            P("dp", "sp", None),
            P("dp", "sp"),
            P("dp", "sp", None),
            P("sp"),
            P("sp", "tp"),
            P("sp", "tp"),
            P("sp", "tp"),
            P(),
            P(None, "tp"),
            P(None, "tp"),
            P(None, "tp"),
            P("tp", None),
            P(),
            P(),
            P("tp"),
        ),
        out_specs=P("dp", "sp", None),
        check_vma=False,
    )
```

```python
import functools
import math

import jax
import jax.numpy as jnp
from jax import lax
from jax.experimental import pallas as pl
from jax.experimental.pallas import tpu as pltpu
from jax.sharding import PartitionSpec as P

GRID_W = 64
norm_eps = 1e-06
rope_base = 10000.0
F32 = jnp.float32
BF16 = jnp.bfloat16
LANES = 128
LOG2E = math.log2(math.e)
GROUP = 2
SCOPED_KIB = 64384


def tables(first, rows, head_dim):
    quarter = head_dim // 4
    half = head_dim // 2
    shape = (rows, 2 * head_dim)
    token = first + lax.broadcasted_iota(jnp.int32, shape, 0)
    lane = lax.broadcasted_iota(jnp.int32, shape, 1) % head_dim
    pair = lane % half
    index = (pair % quarter).astype(F32)
    place = jnp.where(pair < quarter, token // GRID_W, token % GRID_W).astype(F32)
    angle = place * jnp.exp(index * (-math.log(rope_base) / quarter))
    sine = jnp.sin(angle)
    return jnp.cos(angle), jnp.where(lane < half, -sine, sine)


def kernel(
    sizes,
    condition_h, code_h, gain_h, q_gain_h, k_gain_h, bias_h,
    latent, context, shift_w, scale_w, gate_w, wq, wk, wv, wo,
    out,
    condition, code, gain_ref, q_gain, k_gain, bias_ref,
    modw, lat, ctx, wq_v, wkv, wkv_t, wbuf,
    vec_z, vec_t, gate_z, gate_t, normed_c, normed_l, kvbuf, vals, q_s, m_s, acc, att, mixed, cos_s, sin_s, inv_s,
    local, met, sent, came, kv_send, kv_recv, w_recv, x_recv, s_recv, f_recv, a_recv,
):
    n_sp, n_tp, n_dp = sizes
    sp, tp, dp = lax.axis_index("sp"), lax.axis_index("tp"), lax.axis_index("dp")
    rows, crows = lat.shape[0], ctx.shape[0]
    hd = wk.shape[0]
    qcols = wq_v.shape[1]
    heads = qcols // hd
    width = lat.shape[1]
    cols = width // n_tp
    side = cols // 2
    chip = cols // 4
    mid = rows // 2
    lanes = 2 * hd
    dots = functools.partial(jnp.dot, preferred_element_type=F32)
    dims = (((1,), (1,)), ((), ()))
    scope = jax.named_scope

    barrier = pltpu.get_barrier_semaphore()

    def greet(sem, **where):
        pl.semaphore_signal(sem, inc=1, device_id=where, device_id_type=pl.DeviceIdType.MESH)

    for d in range(1, n_sp):
        greet(barrier, sp=(sp + d) % n_sp)
    for d in range(1, n_tp):
        greet(barrier, tp=tp ^ d)
    for d in range(1, n_dp):
        @pl.when(dp + d < n_dp)
        def _():
            greet(barrier, dp=dp + d)

    copies = {}

    def load(number, name, src, dst):
        copies[name] = pltpu.make_async_copy(src, dst, local.at[number])
        copies[name].start()

    load(0, "condition", condition_h, condition)
    load(1, "code", code_h, code)
    load(2, "m0", shift_w, modw.at[0])
    load(3, "m1", scale_w, modw.at[1])
    load(4, "m2", gate_w, modw.at[2])
    load(5, "ctx", context.at[0], ctx)
    load(6, "wk", wk, wkv.at[:hd])
    load(6, "wv", wv, wkv.at[hd:])
    load(7, "lat", latent.at[0], lat)

    def drain(ref, sem):
        pltpu.make_async_copy(ref, ref, sem).wait()

    def remote(src, dst, s, r, **where):
        return pltpu.make_async_remote_copy(
            src_ref=src, dst_ref=dst, send_sem=s, recv_sem=r,
            device_id=where, device_id_type=pl.DeviceIdType.MESH)

    with scope("modmat"):
        copies["condition"].wait()
        copies["code"].wait()
        row8 = lax.broadcasted_iota(jnp.int32, (8, condition.shape[1]), 0)
        own_code = condition[...].astype(F32)
        shared_code = code[...].astype(F32)[None]
        both = jnp.where(row8 == 0, own_code, jnp.where(row8 == 1, shared_code, 0.0))
        both = (both / (1.0 + jnp.exp(-both))).astype(BF16)
        pieces = []
        for k in range(2):
            copies[f"m{k}"].wait()
            pieces.append(dots(both, modw[k])[:2])
        rows4 = jnp.concatenate(pieces, axis=0)
        vec_z[sp] = jnp.concatenate([rows4[:, :side], rows4[:, side:]], axis=0)

    load(0, "gain", gain_h, gain_ref)
    load(1, "k_gain", k_gain_h, k_gain)
    load(2, "wq", wq, wq_v)
    load(3, "wo", wo, wbuf.at[tp])

    with scope("barrier"):
        pl.semaphore_wait(barrier, n_sp + n_tp - 2 + dp)

    for d in range(1, n_sp):
        remote(vec_z.at[sp], vec_z.at[sp], sent.at[0], came.at[0], sp=(sp + d) % n_sp).start()
    for d in range(1, n_dp):
        @pl.when(dp - d >= 0)
        def _():
            greet(met, dp=dp - d)

    share = wo.shape[0] // n_dp
    piece = share // 8
    near = [d for d in (1, 2) if d < n_tp]
    paired = n_sp % 2 == 0
    turns = {1: ((3, 1), (4, 2), (0, 3)), 2: ((0, 1), (1, 2), (3, 3))}

    def span(core, first, count):
        return pl.ds(pl.multiple_of(core * share + first * piece, piece), count * piece)

    def extra(core, plane):
        if paired:
            return span(core, 6 + plane % 2, 1)
        return span(core, 6, 2)

    def send_weights(d, turn):
        area = extra(dp, sp) if turn == 3 else span(dp, *turns[d][turn])
        remote(wo.at[area], wbuf.at[tp, area], sent.at[4], w_recv.at[d - 1, turn], tp=tp ^ d).start()

    def share_weights(ref):
        for e in range(1, n_dp):
            remote(ref, ref, sent.at[5], f_recv.at[e - 1], dp=(dp + e) % n_dp).start()

    def got_weights(d, turn):
        ref = wbuf.at[tp ^ d, span(dp, *turns[d][turn])]
        drain(ref, w_recv.at[d - 1, turn])
        if n_tp == 4 and turn < 2:
            remote(ref, ref, sent.at[4], x_recv.at[d - 1], tp=tp ^ (3 - d)).start()
        share_weights(ref)

    def across(d):
        ref = wbuf.at[tp ^ d, extra(dp, sp)]
        if paired:
            remote(ref, ref, sent.at[4], s_recv.at[d // 3], sp=sp ^ 1).start()

    def got_extra():
        for d in near:
            ref = wbuf.at[tp ^ d, extra(dp, sp)]
            drain(ref, w_recv.at[d - 1, 3])
            if n_tp == 4:
                @pl.when(dp % 2 == 2 - d)
                def _():
                    remote(ref, ref, sent.at[4], x_recv.at[2], tp=tp ^ (3 - d)).start()
            across(d)

    def share_extra():
        for d in near:
            share_weights(wbuf.at[tp ^ d, extra(dp, sp)])

    def got_extra_far():
        ref = wbuf.at[tp ^ 3, extra(dp, sp)]
        drain(ref, x_recv.at[2])
        across(3)
        share_weights(ref)

    def got_across(far):
        if paired:
            area = extra(dp, sp + 1)
            those = [3] if far else near
            drain(wbuf.at[:len(those), area], s_recv.at[1 if far else 0])
            for d in those:
                share_weights(wbuf.at[tp ^ d, area])

    def got_far():
        for d in near:
            ref = wbuf.at[tp ^ 3, span(dp, turns[d][0][0], 3)]
            drain(ref, x_recv.at[d - 1])
            share_weights(ref)

    for turn in (3, 0):
        for d in near:
            send_weights(d, turn)

    with scope("gate"):
        copies["m2"].wait()
        row = dots(both, modw[2])[:1]
        gate_z[sp] = jnp.concatenate([row[:, j * chip:(j + 1) * chip] for j in range(4)], axis=0)
    for d in range(1, n_sp):
        remote(gate_z.at[sp], gate_z.at[sp], sent.at[2], came.at[2], sp=(sp + d) % n_sp).start()

    with scope("tables"):
        cosine, sine = tables(sp * rows, rows, hd)
        cos_s[...] = cosine
        sin_s[...] = sine
    with scope("inv"):
        copies["ctx"].wait()
        floats = ctx[...].astype(F32)
        inv_c = lax.rsqrt(jnp.mean(floats * floats, axis=-1, keepdims=True) + norm_eps)
        copies["lat"].wait()
        floats = lat[...].astype(F32)
        inv_s[...] = lax.rsqrt(jnp.mean(floats * floats, axis=-1, keepdims=True) + norm_eps)

    with scope("turn"):
        drain(wkv, local.at[6])
        for d in range(n_tp):
            wkv_t[d * cols:(d + 1) * cols] = wkv[:, pl.ds(pl.multiple_of((tp ^ d) * cols, cols), cols)].T
    with scope("zwait"):
        if n_sp > 1:
            drain(vec_z.at[:n_sp - 1], came.at[0])
    total = vec_z[0]
    for k in range(1, n_sp):
        total = total + vec_z[k]
    vec_t[tp] = total
    for d in reversed(range(1, n_tp)):
        remote(vec_t.at[tp], vec_t.at[tp], sent.at[1], came.at[1 if d in near else 4], tp=tp ^ d).start()
    with scope("extra"):
        got_extra()
    for turn in (1, 2):
        for d in near:
            send_weights(d, turn)
    early, far = [0] + near, list(range(3, n_tp))
    cut = len(early) * cols

    def modulate(tokens, inverse, which, normed, offsets):
        for d in offsets:
            t = tp ^ d
            for k in range(2):
                part = pl.ds(pl.multiple_of(t * cols + k * side, side), side)
                at = 4 * k + which
                factor = gain_ref[:, part] * (1.0 + vec_t[t, at + 2:at + 3, :])
                shift = vec_t[t, at:at + 1, :]
                values = tokens[:, part].astype(F32) * inverse * factor + shift
                normed[:, d * cols + k * side:d * cols + (k + 1) * side] = values.astype(BF16)

    def kv_copy(block, target, way, part):
        area = pl.ds(0, crows) if part == 0 else pl.ds(crows, rows)
        ref = kvbuf.at[block, area]
        return remote(ref, ref, kv_send.at[0], kv_recv.at[part, block], sp=target)

    def send_own(part):
        @pl.when(sp + 1 < n_sp)
        def _():
            kv_copy(sp, sp + 1, 0, part).start()

        @pl.when(sp > 0)
        def _():
            kv_copy(sp, sp - 1, 1, part).start()

    def send_far(part):
        if n_sp > 2:
            @pl.when(sp == 0)
            def _():
                kv_copy(sp, n_sp - 1, 1, part).start()

            @pl.when(sp == n_sp - 1)
            def _():
                kv_copy(sp, 0, 0, part).start()

    def averages(values):
        n = values.shape[1]
        row = lax.broadcasted_iota(jnp.int32, (n, n), 0) // hd
        col = lax.broadcasted_iota(jnp.int32, (n, n), 1) // hd
        spread = jnp.where(row == col, 1.0 / hd, 0.0).astype(BF16)
        return dots((values * values).astype(BF16), spread)

    def swapped(values):
        lane = lax.broadcasted_iota(jnp.int32, values.shape, 1) % hd
        return jnp.where(lane < hd // 2, pltpu.roll(values, lanes - hd // 2, 1), pltpu.roll(values, hd // 2, 1))

    def key_values(kv, turn):
        lane = lax.broadcasted_iota(jnp.int32, kv.shape, 1)
        keys = kv * lax.rsqrt(averages(kv) + norm_eps) * jnp.concatenate([k_gain[...]] * 2, axis=1)
        if turn:
            keys = keys * cos_s[...] + swapped(keys) * sin_s[...]
        return jnp.where(lane < hd, keys, kv).astype(BF16)

    copies["gain"].wait()
    copies["k_gain"].wait()
    load(0, "q_gain", q_gain_h, q_gain)
    load(1, "bias", bias_h, bias_ref)
    with scope("twait1"):
        if near:
            drain(vec_t.at[:len(near)], came.at[1])
    with scope("modctx"):
        modulate(ctx, inv_c, 1, normed_c, early)
        partial = dots(normed_c[:, :cut], wkv_t[:cut])
        modulate(lat, inv_s[...], 0, normed_l, early)
    with scope("twait2"):
        for d in far:
            drain(vec_t.at[tp ^ d], came.at[4])
    with scope("kvctx"):
        if far:
            modulate(ctx, inv_c, 1, normed_c, far)
            partial = partial + dots(normed_c[:, cut:], wkv_t[cut:])
        kvbuf[sp, :crows] = key_values(partial, False)
    send_far(0)
    send_own(0)

    with scope("kvlat"):
        modulate(lat, inv_s[...], 0, normed_l, far)
        kvbuf[sp, crows:] = key_values(dots(normed_l[...], wkv_t[...]), True)
    send_far(1)
    send_own(1)

    with scope("gotw0"):
        for d in range(1, n_dp):
            @pl.when(dp + d < n_dp)
            def _():
                pl.semaphore_wait(met, 1)
        for d in near:
            got_weights(d, 0)
        share_extra()

    with scope("qproj"):
        copies["wq"].wait()
        copies["q_gain"].wait()
        queries = functools.reduce(jnp.add, [
            dots(normed_l[:, d * cols:(d + 1) * cols], wq_v[pl.ds(pl.multiple_of((tp ^ d) * cols, cols), cols)])
            for d in range(n_tp)])
        factor = lax.rsqrt(averages(queries) + norm_eps)
        gains = jnp.concatenate([q_gain[...]] * 2, axis=1) * (hd ** -0.5 * LOG2E)
        lane = lax.broadcasted_iota(jnp.int32, (rows, lanes), 1)
        for g in range(heads // 2):
            pair = slice(g * lanes, (g + 1) * lanes)
            two = queries[:, pair] * factor[:, pair] * gains
            two = two * cos_s[...] + swapped(two) * sin_s[...]
            for h, one in ((2 * g, two), (2 * g + 1, pltpu.roll(two, hd, 1))):
                one = jnp.where(lane < hd, one, 0.0).astype(BF16)
                for half in range(2):
                    q_s[half, h * mid:(h + 1) * mid] = one[half * mid:(half + 1) * mid]

    with scope("gatez"):
        if n_sp > 1:
            drain(gate_z.at[:n_sp - 1], came.at[2])
        total = gate_z[0]
        for k in range(1, n_sp):
            total = total + gate_z[k]
        gate_t[tp] = total
    for d in range(1, n_tp):
        remote(gate_t.at[tp], gate_t.at[tp], sent.at[3], came.at[3], tp=tp ^ d).start()

    def spread(column, count):
        if count % LANES == 0:
            return jnp.concatenate([column] * (count // LANES), axis=1)
        return column[:, :count]

    def prepare(block):
        pairs = kvbuf[block]
        lane = lax.broadcasted_iota(jnp.int32, pairs.shape, 1)
        vals[...] = jnp.where(lane < hd, jnp.ones_like(pairs), pairs)

    def absorb(block, half, first=False):
        def scores(g):
            query = q_s[half, g * GROUP * mid:(g + 1) * GROUP * mid]
            return (lax.dot_general(query, kvbuf[block, :crows], dims, preferred_element_type=F32),
                    lax.dot_general(query, kvbuf[block, crows:], dims, preferred_element_type=F32))

        ahead = scores(0)
        for g in range(heads // GROUP):
            all_c, all_l = ahead
            if (g + 1) * GROUP < heads:
                ahead = scores(g + 1)
            shares, weights_c, weights_l = [], [], []
            for k in range(GROUP):
                h = g * GROUP + k
                s_c, s_l = all_c[k * mid:(k + 1) * mid], all_l[k * mid:(k + 1) * mid]
                bias = bias_ref[h] * LOG2E
                top = jnp.maximum(s_c.max(axis=1, keepdims=True) + bias, s_l.max(axis=1, keepdims=True))
                top = jnp.broadcast_to(top, (mid, lanes))
                new = top if first else jnp.maximum(m_s[half, h], top)
                weights_c.append(jnp.exp2(s_c - spread(new - bias, crows)).astype(BF16))
                weights_l.append(jnp.exp2(s_l - spread(new, rows)).astype(BF16))
                shares.append(None if first else jnp.exp2(m_s[half, h] - new))
                m_s[half, h] = new
            more = (dots(jnp.concatenate(weights_c, axis=0), vals[:crows])
                    + dots(jnp.concatenate(weights_l, axis=0), vals[crows:]))
            for k in range(GROUP):
                h = g * GROUP + k
                own = more[k * mid:(k + 1) * mid]
                acc[half, h] = own if first else acc[half, h] * shares[k] + own

    def absorb_all(block, first=False):
        prepare(block)

        @pl.loop(0, 2)
        def _(half):
            absorb(block, half, first)

    lower = 2 * sp < n_sp
    edge = (sp == 0) | (sp == n_sp - 1)

    def away(s):
        if n_sp < 3:
            return s
        return jnp.where(edge & (s > 1), jnp.where(s == 2, n_sp - 1, s - 1), s)

    reach = jnp.where(edge, away(n_sp - 1), jnp.where(lower, n_sp - 1 - sp, sp))
    last = jnp.where(lower, sp + reach, sp - reach)

    def passes(block, target):
        if n_sp < 3:
            return (target >= 0) & (target < n_sp)
        far = ((block == 0) & (target == n_sp - 1)) | ((block == n_sp - 1) & (target == 0))
        return (target >= 0) & (target < n_sp) & jnp.logical_not(far)

    def forward(s, parts=(0, 1)):
        d = away(s)
        for part in parts:
            @pl.when(sp - d >= 0)
            def _():
                kv_copy(sp - d, sp, 0, part).wait_recv()

                @pl.when(passes(sp - d, sp + 1))
                def _():
                    kv_copy(sp - d, sp + 1, 0, part).start()

            @pl.when(sp + d < n_sp)
            def _():
                kv_copy(sp + d, sp, 1, part).wait_recv()

                @pl.when(passes(sp + d, sp - 1))
                def _():
                    kv_copy(sp + d, sp - 1, 1, part).start()

    copies["bias"].wait()
    with scope("absorb0"):
        prepare(sp)
        absorb(sp, 0, True)
    with scope("got1"):
        for d in near:
            got_weights(d, 1)
    if n_sp > 1:
        with scope("fwd1c"):
            forward(1, (0,))
    with scope("absorb0"):
        absorb(sp, 1, True)
    if n_sp > 1:
        with scope("fwd1l"):
            forward(1, (1,))
    def side_block(s, long):
        block = jnp.where(lower == long, sp + away(s), sp - away(s))

        @pl.when((block >= 0) & (block < n_sp) & (block != last))
        def _():
            with scope("absorb"):
                absorb_all(block)

    @pl.loop(1, n_sp)
    def _(s):
        def onward():
            @pl.when(s + 1 < n_sp)
            def _():
                with scope("fwd"):
                    forward(s + 1)

        side_block(s, True)
        if n_sp > 4:
            onward()
        side_block(s, False)
        if n_sp <= 4:
            onward()

    if n_tp == 4:
        @pl.when(dp == 0)
        def _():
            got_extra_far()

    if n_sp > 1:
        with scope("prepare"):
            prepare(last)
    lane = lax.broadcasted_iota(jnp.int32, (mid, lanes), 1)
    for half in range(2):
        if n_sp > 1:
            with scope("final"):
                absorb(last, half)
        for g in range(heads // 2):
            even, odd = acc[half, 2 * g], acc[half, 2 * g + 1]
            top = jnp.where(lane < hd, pltpu.roll(even, hd, 1), odd)
            low = jnp.where(lane < hd, even, pltpu.roll(odd, hd, 1))
            att[tp, half, :, g * lanes:(g + 1) * lanes] = (top / low).astype(BF16)
        for d in reversed(range(1, n_tp)):
            remote(att.at[tp, half], att.at[tp, half], sent.at[6], a_recv.at[half * d], tp=tp ^ d).start()

    with scope("gotw1"):
        if n_tp == 4:
            @pl.when(dp > 0)
            def _():
                got_extra_far()
        for d in near:
            got_weights(d, 2)
        if near:
            got_across(False)
    copies["wo"].wait()

    def project(group, half, part):
        return dots(att[group, half], wbuf[group, :, part])

    parts = [slice(t * cols, (t + 1) * cols) for t in range(n_tp)]
    tall = [slice(half * mid, (half + 1) * mid) for half in range(2)]
    with scope("own"):
        for half in range(2):
            for part in parts:
                mixed[tall[half], part] = project(tp, half, part)

    with scope("gotw3"):
        if n_tp == 4:
            got_far()
            got_across(True)
        for e in range(1, n_dp):
            if n_tp > 1:
                drain(wbuf.at[:n_tp - 1, :share], f_recv.at[e - 1])
        if n_tp > 1:
            drain(gate_t.at[:n_tp - 1], came.at[3])

    order = [d for d in (1, 3, 2) if d < n_tp]
    for half in range(2):
        for d in order:
            with scope(f"att{half}{d}"):
                if half == 0 and d == order[0]:
                    drain(att.at[:n_tp - 1, 0], a_recv.at[0])
                if half == 1:
                    drain(att.at[tp ^ d, 1], a_recv.at[d])
            if d != order[-1]:
                for part in parts:
                    mixed[tall[half], part] = mixed[tall[half], part] + project(tp ^ d, half, part)
        for t, part in enumerate(parts):
            value = mixed[tall[half], part]
            if order:
                value = value + project(tp ^ order[-1], half, part)
            gate = jnp.concatenate([gate_t[t, j:j + 1, :] for j in range(4)], axis=1)
            out[0, tall[half], part] = (lat[tall[half], part].astype(F32) + gate * value).astype(BF16)

    with scope("sendwait"):
        if n_sp > 1:
            drain(vec_z.at[:n_sp - 1], sent.at[0])
            drain(gate_z.at[:n_sp - 1], sent.at[2])
        if n_tp > 1:
            drain(vec_t.at[:n_tp - 1], sent.at[1])
            drain(gate_t.at[:n_tp - 1], sent.at[3])
            drain(wbuf.at[:n_tp - 1, :share], sent.at[4])
            for e in range(1, n_dp):
                drain(wbuf.at[:n_tp - 1, :share], sent.at[5])
            drain(att.at[:n_tp - 1], sent.at[6])

        if n_sp == 2:
            drain(kvbuf.at[:1], kv_send.at[0])
        if n_sp > 2:
            fewer = (sp == 1).astype(jnp.int32) + (sp == n_sp - 2).astype(jnp.int32)

            @pl.when(edge)
            def _():
                drain(kvbuf.at[:2], kv_send.at[0])

            for less in range(3):
                @pl.when(jnp.logical_not(edge) & (fewer == less))
                def _():
                    drain(kvbuf.at[:min(n_sp, n_sp + 1 - less)], kv_send.at[0])
                    if less == 0:
                        drain(kvbuf.at[:1], kv_send.at[0])


def on_device(
    sizes, latent, condition, context, context_code, shift_weight, scale_weight, gate_weight,
    norm_gain, query_weight, key_weight, value_weight, output_weight, query_gain, key_gain,
    context_bias,
):
    n_sp, n_tp, n_dp = sizes
    rows, width = latent.shape[1:]
    crows = context.shape[1]
    hd = query_gain.shape[0]
    qcols = query_weight.shape[1]
    heads = qcols // hd
    deep, cols = shift_weight.shape
    vmem = pl.BlockSpec(memory_space=pltpu.VMEM)
    hbm = pl.BlockSpec(memory_space=pl.ANY)
    dma = pltpu.SemaphoreType.DMA
    mid = rows // 2
    lanes = 2 * hd
    scratch = [
        pltpu.VMEM((1, deep), BF16), pltpu.VMEM((deep,), BF16), pltpu.VMEM((1, width), F32),
        pltpu.VMEM((1, hd), F32), pltpu.VMEM((1, hd), F32), pltpu.SMEM((heads,), F32),
        pltpu.VMEM((3, deep, cols), BF16),
        pltpu.VMEM((rows, width), BF16),
        pltpu.VMEM((crows, width), BF16),
        pltpu.VMEM((width, qcols), BF16),
        pltpu.VMEM((lanes, width), BF16),
        pltpu.VMEM((width, lanes), BF16),
        pltpu.VMEM((n_tp,) + output_weight.shape, BF16),
        pltpu.VMEM((n_sp, 8, cols // 2), F32),
        pltpu.VMEM((n_tp, 8, cols // 2), F32),
        pltpu.VMEM((n_sp, 4, cols // 4), F32),
        pltpu.VMEM((n_tp, 4, cols // 4), F32),
        pltpu.VMEM((crows, width), BF16),
        pltpu.VMEM((rows, width), BF16),
        pltpu.VMEM((n_sp, crows + rows, lanes), BF16),
        pltpu.VMEM((crows + rows, lanes), BF16),
        pltpu.VMEM((2, heads * mid, lanes), BF16),
        pltpu.VMEM((2, heads, mid, lanes), F32),
        pltpu.VMEM((2, heads, mid, lanes), F32),
        pltpu.VMEM((n_tp, 2, mid, qcols), BF16),
        pltpu.VMEM((rows, width), F32),
        pltpu.VMEM((rows, lanes), F32),
        pltpu.VMEM((rows, lanes), F32),
        pltpu.VMEM((rows, 1), F32),
        dma((8,)), pltpu.SemaphoreType.REGULAR, dma((7,)), dma((5,)),
        dma((1,)), dma((2, n_sp)), dma((2, 4)), dma((3,)), dma((2,)), dma((max(1, n_dp - 1),)), dma((n_tp,)),
    ]
    return pl.pallas_call(
        functools.partial(kernel, sizes),
        out_shape=pltpu.VMEM(latent.shape, BF16),
        in_specs=[hbm] * 15,
        out_specs=vmem,
        scratch_shapes=scratch,
        compiler_params=pltpu.CompilerParams(
            collective_id=0, has_side_effects=True, vmem_limit_bytes=SCOPED_KIB * 1024),
    )(
        condition, context_code, norm_gain[None], query_gain[None], key_gain[None],
        context_bias, latent, context, shift_weight, scale_weight, gate_weight, query_weight,
        key_weight.T, value_weight.T, output_weight,
    )


def solution(mesh):
    sizes = tuple(mesh.shape[axis] for axis in ("sp", "tp", "dp"))
    return jax.shard_map(
        functools.partial(on_device, sizes),
        mesh=mesh,
        in_specs=(
            P("dp", "sp", None),
            P("dp", "sp"),
            P("dp", "sp", None),
            P("sp"),
            P("sp", "tp"),
            P("sp", "tp"),
            P("sp", "tp"),
            P(),
            P(None, "tp"),
            P(None, "tp"),
            P(None, "tp"),
            P("tp", None),
            P(),
            P(),
            P("tp"),
        ),
        out_specs=P("dp", "sp", None),
        check_vma=False,
    )
```

```python
import functools
import math

import jax
import jax.numpy as jnp
from jax import lax
from jax.experimental import pallas as pl
from jax.experimental.pallas import tpu as pltpu
from jax.sharding import PartitionSpec as P

GRID_W = 64
norm_eps = 1e-06
rope_base = 10000.0
F32 = jnp.float32
BF16 = jnp.bfloat16
LANES = 128
LOG2E = math.log2(math.e)
GROUP = 2
SCOPED_KIB = 64384


def tables(first, rows, head_dim):
    quarter = head_dim // 4
    half = head_dim // 2
    shape = (rows, 2 * head_dim)
    token = first + lax.broadcasted_iota(jnp.int32, shape, 0)
    lane = lax.broadcasted_iota(jnp.int32, shape, 1) % head_dim
    pair = lane % half
    index = (pair % quarter).astype(F32)
    place = jnp.where(pair < quarter, token // GRID_W, token % GRID_W).astype(F32)
    angle = place * jnp.exp(index * (-math.log(rope_base) / quarter))
    sine = jnp.sin(angle)
    return jnp.cos(angle), jnp.where(lane < half, -sine, sine)


def kernel(
    sizes,
    condition_h, code_h, gain_h, q_gain_h, k_gain_h, bias_h,
    latent, context, shift_w, scale_w, gate_w, wq, wk, wv, wo,
    out,
    condition, code, gain_ref, q_gain, k_gain, bias_ref,
    modw, lat, ctx, wq_v, wkv, wkv_t, wbuf,
    vec_z, vec_t, gate_z, gate_t, normed_c, normed_l, kvbuf, vals, q_s, m_s, acc, att, mixed, cos_s, sin_s, inv_s,
    local, met, sent, came, kv_send, kv_recv, w_recv, x_recv, s_recv, f_recv, a_recv,
):
    n_sp, n_tp, n_dp = sizes
    sp, tp, dp = lax.axis_index("sp"), lax.axis_index("tp"), lax.axis_index("dp")
    rows, crows = lat.shape[0], ctx.shape[0]
    hd = wk.shape[0]
    qcols = wq_v.shape[1]
    heads = qcols // hd
    width = lat.shape[1]
    cols = width // n_tp
    side = cols // 2
    chip = cols // 4
    mid = rows // 2
    lanes = 2 * hd
    dots = functools.partial(jnp.dot, preferred_element_type=F32)
    dims = (((1,), (1,)), ((), ()))
    scope = jax.named_scope

    barrier = pltpu.get_barrier_semaphore()

    def greet(sem, **where):
        pl.semaphore_signal(sem, inc=1, device_id=where, device_id_type=pl.DeviceIdType.MESH)

    for d in range(1, n_sp):
        greet(barrier, sp=(sp + d) % n_sp)
    for d in range(1, n_tp):
        greet(barrier, tp=tp ^ d)
    for d in range(1, n_dp):
        @pl.when(dp + d < n_dp)
        def _():
            greet(barrier, dp=dp + d)

    copies = {}

    def load(number, name, src, dst):
        copies[name] = pltpu.make_async_copy(src, dst, local.at[number])
        copies[name].start()

    load(0, "condition", condition_h, condition)
    load(1, "code", code_h, code)
    load(2, "m0", shift_w, modw.at[0])
    load(3, "m1", scale_w, modw.at[1])
    load(4, "m2", gate_w, modw.at[2])
    load(5, "ctx", context.at[0], ctx)
    load(6, "wk", wk, wkv.at[:hd])
    load(6, "wv", wv, wkv.at[hd:])
    load(7, "lat", latent.at[0], lat)

    def drain(ref, sem):
        pltpu.make_async_copy(ref, ref, sem).wait()

    def remote(src, dst, s, r, **where):
        return pltpu.make_async_remote_copy(
            src_ref=src, dst_ref=dst, send_sem=s, recv_sem=r,
            device_id=where, device_id_type=pl.DeviceIdType.MESH)

    with scope("modmat"):
        copies["condition"].wait()
        copies["code"].wait()
        row8 = lax.broadcasted_iota(jnp.int32, (8, condition.shape[1]), 0)
        own_code = condition[...].astype(F32)
        shared_code = code[...].astype(F32)[None]
        both = jnp.where(row8 == 0, own_code, jnp.where(row8 == 1, shared_code, 0.0))
        both = (both / (1.0 + jnp.exp(-both))).astype(BF16)
        pieces = []
        for k in range(2):
            copies[f"m{k}"].wait()
            pieces.append(dots(both, modw[k])[:2])
        rows4 = jnp.concatenate(pieces, axis=0)
        vec_z[sp] = jnp.concatenate([rows4[:, :side], rows4[:, side:]], axis=0)

    load(0, "gain", gain_h, gain_ref)
    load(1, "k_gain", k_gain_h, k_gain)
    load(2, "wq", wq, wq_v)
    load(3, "wo", wo, wbuf.at[tp])

    with scope("barrier"):
        pl.semaphore_wait(barrier, n_sp + n_tp - 2 + dp)

    for d in range(1, n_sp):
        remote(vec_z.at[sp], vec_z.at[sp], sent.at[0], came.at[0], sp=(sp + d) % n_sp).start()
    for d in range(1, n_dp):
        @pl.when(dp - d >= 0)
        def _():
            greet(met, dp=dp - d)

    share = wo.shape[0] // n_dp
    piece = share // 8
    near = [d for d in (1, 2) if d < n_tp]
    paired = n_sp % 2 == 0
    turns = {1: ((3, 1), (4, 2), (0, 3)), 2: ((0, 1), (1, 2), (3, 3))}

    def span(core, first, count):
        return pl.ds(pl.multiple_of(core * share + first * piece, piece), count * piece)

    def extra(core, plane):
        if paired:
            return span(core, 6 + plane % 2, 1)
        return span(core, 6, 2)

    def send_weights(d, turn):
        area = extra(dp, sp) if turn == 3 else span(dp, *turns[d][turn])
        remote(wo.at[area], wbuf.at[tp, area], sent.at[4], w_recv.at[d - 1, turn], tp=tp ^ d).start()

    def share_weights(ref):
        for e in range(1, n_dp):
            remote(ref, ref, sent.at[5], f_recv.at[e - 1], dp=(dp + e) % n_dp).start()

    def got_weights(d, turn):
        ref = wbuf.at[tp ^ d, span(dp, *turns[d][turn])]
        drain(ref, w_recv.at[d - 1, turn])
        if n_tp == 4 and turn < 2:
            remote(ref, ref, sent.at[4], x_recv.at[d - 1], tp=tp ^ (3 - d)).start()
        share_weights(ref)

    def across(d):
        ref = wbuf.at[tp ^ d, extra(dp, sp)]
        if paired:
            remote(ref, ref, sent.at[4], s_recv.at[d // 3], sp=sp ^ 1).start()

    def got_extra():
        for d in near:
            ref = wbuf.at[tp ^ d, extra(dp, sp)]
            drain(ref, w_recv.at[d - 1, 3])
            if n_tp == 4:
                @pl.when(dp % 2 == 2 - d)
                def _():
                    remote(ref, ref, sent.at[4], x_recv.at[2], tp=tp ^ (3 - d)).start()
            across(d)

    def share_extra():
        for d in near:
            share_weights(wbuf.at[tp ^ d, extra(dp, sp)])

    def got_extra_far():
        ref = wbuf.at[tp ^ 3, extra(dp, sp)]
        drain(ref, x_recv.at[2])
        across(3)
        share_weights(ref)

    def got_across(far):
        if paired:
            area = extra(dp, sp + 1)
            those = [3] if far else near
            drain(wbuf.at[:len(those), area], s_recv.at[1 if far else 0])
            for d in those:
                share_weights(wbuf.at[tp ^ d, area])

    def got_far():
        for d in near:
            ref = wbuf.at[tp ^ 3, span(dp, turns[d][0][0], 3)]
            drain(ref, x_recv.at[d - 1])
            share_weights(ref)

    for turn in (3, 0):
        for d in near:
            send_weights(d, turn)

    with scope("gate"):
        copies["m2"].wait()
        row = dots(both, modw[2])[:1]
        gate_z[sp] = jnp.concatenate([row[:, j * chip:(j + 1) * chip] for j in range(4)], axis=0)
    for d in range(1, n_sp):
        remote(gate_z.at[sp], gate_z.at[sp], sent.at[2], came.at[2], sp=(sp + d) % n_sp).start()

    with scope("tables"):
        cosine, sine = tables(sp * rows, rows, hd)
        cos_s[...] = cosine
        sin_s[...] = sine
    with scope("inv"):
        copies["ctx"].wait()
        floats = ctx[...].astype(F32)
        inv_c = lax.rsqrt(jnp.mean(floats * floats, axis=-1, keepdims=True) + norm_eps)
        copies["lat"].wait()
        floats = lat[...].astype(F32)
        inv_s[...] = lax.rsqrt(jnp.mean(floats * floats, axis=-1, keepdims=True) + norm_eps)

    with scope("turn"):
        drain(wkv, local.at[6])
        for d in range(n_tp):
            wkv_t[d * cols:(d + 1) * cols] = wkv[:, pl.ds(pl.multiple_of((tp ^ d) * cols, cols), cols)].T
    with scope("zwait"):
        if n_sp > 1:
            drain(vec_z.at[:n_sp - 1], came.at[0])
    total = vec_z[0]
    for k in range(1, n_sp):
        total = total + vec_z[k]
    vec_t[tp] = total
    for d in reversed(range(1, n_tp)):
        remote(vec_t.at[tp], vec_t.at[tp], sent.at[1], came.at[1 if d in near else 4], tp=tp ^ d).start()
    with scope("extra"):
        got_extra()
    for turn in (1, 2):
        for d in near:
            send_weights(d, turn)
    early, far = [0] + near, list(range(3, n_tp))
    cut = len(early) * cols

    def modulate(tokens, inverse, which, normed, offsets):
        for d in offsets:
            t = tp ^ d
            for k in range(2):
                part = pl.ds(pl.multiple_of(t * cols + k * side, side), side)
                at = 4 * k + which
                factor = gain_ref[:, part] * (1.0 + vec_t[t, at + 2:at + 3, :])
                shift = vec_t[t, at:at + 1, :]
                values = tokens[:, part].astype(F32) * inverse * factor + shift
                normed[:, d * cols + k * side:d * cols + (k + 1) * side] = values.astype(BF16)

    def kv_copy(block, target, way, part):
        area = pl.ds(0, crows) if part == 0 else pl.ds(crows, rows)
        ref = kvbuf.at[block, area]
        return remote(ref, ref, kv_send.at[0], kv_recv.at[part, block], sp=target)

    def send_own(part):
        @pl.when(sp + 1 < n_sp)
        def _():
            kv_copy(sp, sp + 1, 0, part).start()

        @pl.when(sp > 0)
        def _():
            kv_copy(sp, sp - 1, 1, part).start()

    def send_far(part):
        if n_sp > 2:
            @pl.when(sp == 0)
            def _():
                kv_copy(sp, n_sp - 1, 1, part).start()

            @pl.when(sp == n_sp - 1)
            def _():
                kv_copy(sp, 0, 0, part).start()

    def averages(values):
        n = values.shape[1]
        row = lax.broadcasted_iota(jnp.int32, (n, n), 0) // hd
        col = lax.broadcasted_iota(jnp.int32, (n, n), 1) // hd
        spread = jnp.where(row == col, 1.0 / hd, 0.0).astype(BF16)
        return dots((values * values).astype(BF16), spread)

    def swapped(values):
        lane = lax.broadcasted_iota(jnp.int32, values.shape, 1) % hd
        return jnp.where(lane < hd // 2, pltpu.roll(values, lanes - hd // 2, 1), pltpu.roll(values, hd // 2, 1))

    def key_values(kv, turn):
        lane = lax.broadcasted_iota(jnp.int32, kv.shape, 1)
        keys = kv * lax.rsqrt(averages(kv) + norm_eps) * jnp.concatenate([k_gain[...]] * 2, axis=1)
        if turn:
            keys = keys * cos_s[...] + swapped(keys) * sin_s[...]
        return jnp.where(lane < hd, keys, kv).astype(BF16)

    copies["gain"].wait()
    copies["k_gain"].wait()
    load(0, "q_gain", q_gain_h, q_gain)
    load(1, "bias", bias_h, bias_ref)
    with scope("twait1"):
        if near:
            drain(vec_t.at[:len(near)], came.at[1])
    with scope("modctx"):
        modulate(ctx, inv_c, 1, normed_c, early)
        partial = dots(normed_c[:, :cut], wkv_t[:cut])
        modulate(lat, inv_s[...], 0, normed_l, early)
    with scope("twait2"):
        for d in far:
            drain(vec_t.at[tp ^ d], came.at[4])
    with scope("kvctx"):
        if far:
            modulate(ctx, inv_c, 1, normed_c, far)
            partial = partial + dots(normed_c[:, cut:], wkv_t[cut:])
        kvbuf[sp, :crows] = key_values(partial, False)
    send_far(0)
    send_own(0)

    with scope("kvlat"):
        modulate(lat, inv_s[...], 0, normed_l, far)
        kvbuf[sp, crows:] = key_values(dots(normed_l[...], wkv_t[...]), True)
    send_far(1)
    send_own(1)

    with scope("gotw0"):
        for d in range(1, n_dp):
            @pl.when(dp + d < n_dp)
            def _():
                pl.semaphore_wait(met, 1)
        for d in near:
            got_weights(d, 0)
        share_extra()

    with scope("qproj"):
        copies["wq"].wait()
        copies["q_gain"].wait()
        queries = functools.reduce(jnp.add, [
            dots(normed_l[:, d * cols:(d + 1) * cols], wq_v[pl.ds(pl.multiple_of((tp ^ d) * cols, cols), cols)])
            for d in range(n_tp)])
        factor = lax.rsqrt(averages(queries) + norm_eps)
        gains = jnp.concatenate([q_gain[...]] * 2, axis=1) * (hd ** -0.5 * LOG2E)
        lane = lax.broadcasted_iota(jnp.int32, (rows, lanes), 1)
        for g in range(heads // 2):
            pair = slice(g * lanes, (g + 1) * lanes)
            two = queries[:, pair] * factor[:, pair] * gains
            two = two * cos_s[...] + swapped(two) * sin_s[...]
            for h, one in ((2 * g, two), (2 * g + 1, pltpu.roll(two, hd, 1))):
                one = jnp.where(lane < hd, one, 0.0).astype(BF16)
                for half in range(2):
                    q_s[half, h * mid:(h + 1) * mid] = one[half * mid:(half + 1) * mid]

    with scope("gatez"):
        if n_sp > 1:
            drain(gate_z.at[:n_sp - 1], came.at[2])
        total = gate_z[0]
        for k in range(1, n_sp):
            total = total + gate_z[k]
        gate_t[tp] = total
    for d in range(1, n_tp):
        remote(gate_t.at[tp], gate_t.at[tp], sent.at[3], came.at[3], tp=tp ^ d).start()

    def spread(column, count):
        if count % LANES == 0:
            return jnp.concatenate([column] * (count // LANES), axis=1)
        return column[:, :count]

    def prepare(block):
        pairs = kvbuf[block]
        lane = lax.broadcasted_iota(jnp.int32, pairs.shape, 1)
        vals[...] = jnp.where(lane < hd, jnp.ones_like(pairs), pairs)

    def absorb(block, half, first=False):
        def scores(g):
            query = q_s[half, g * GROUP * mid:(g + 1) * GROUP * mid]
            return (lax.dot_general(query, kvbuf[block, :crows], dims, preferred_element_type=F32),
                    lax.dot_general(query, kvbuf[block, crows:], dims, preferred_element_type=F32))

        ahead = scores(0)
        for g in range(heads // GROUP):
            all_c, all_l = ahead
            if (g + 1) * GROUP < heads:
                ahead = scores(g + 1)
            shares, weights_c, weights_l = [], [], []
            for k in range(GROUP):
                h = g * GROUP + k
                s_c, s_l = all_c[k * mid:(k + 1) * mid], all_l[k * mid:(k + 1) * mid]
                bias = bias_ref[h] * LOG2E
                top = jnp.maximum(s_c.max(axis=1, keepdims=True) + bias, s_l.max(axis=1, keepdims=True))
                top = jnp.broadcast_to(top, (mid, lanes))
                new = top if first else jnp.maximum(m_s[half, h], top)
                weights_c.append(jnp.exp2(s_c - spread(new - bias, crows)).astype(BF16))
                weights_l.append(jnp.exp2(s_l - spread(new, rows)).astype(BF16))
                shares.append(None if first else jnp.exp2(m_s[half, h] - new))
                m_s[half, h] = new
            more = (dots(jnp.concatenate(weights_c, axis=0), vals[:crows])
                    + dots(jnp.concatenate(weights_l, axis=0), vals[crows:]))
            for k in range(GROUP):
                h = g * GROUP + k
                own = more[k * mid:(k + 1) * mid]
                acc[half, h] = own if first else acc[half, h] * shares[k] + own

    def absorb_all(block, first=False):
        prepare(block)

        @pl.loop(0, 2)
        def _(half):
            absorb(block, half, first)

    lower = 2 * sp < n_sp
    edge = (sp == 0) | (sp == n_sp - 1)

    def away(s):
        if n_sp < 3:
            return s
        return jnp.where(edge & (s > 1), jnp.where(s == 2, n_sp - 1, s - 1), s)

    reach = jnp.where(edge, away(n_sp - 1), jnp.where(lower, n_sp - 1 - sp, sp))
    last = jnp.where(lower, sp + reach, sp - reach)

    def passes(block, target):
        if n_sp < 3:
            return (target >= 0) & (target < n_sp)
        far = ((block == 0) & (target == n_sp - 1)) | ((block == n_sp - 1) & (target == 0))
        return (target >= 0) & (target < n_sp) & jnp.logical_not(far)

    def forward(s, parts=(0, 1)):
        d = away(s)
        for part in parts:
            @pl.when(sp - d >= 0)
            def _():
                kv_copy(sp - d, sp, 0, part).wait_recv()

                @pl.when(passes(sp - d, sp + 1))
                def _():
                    kv_copy(sp - d, sp + 1, 0, part).start()

            @pl.when(sp + d < n_sp)
            def _():
                kv_copy(sp + d, sp, 1, part).wait_recv()

                @pl.when(passes(sp + d, sp - 1))
                def _():
                    kv_copy(sp + d, sp - 1, 1, part).start()

    copies["bias"].wait()
    with scope("absorb0"):
        prepare(sp)
        absorb(sp, 0, True)
    with scope("got1"):
        for d in near:
            got_weights(d, 1)
    if n_sp > 1:
        with scope("fwd1c"):
            forward(1, (0,))
    with scope("absorb0"):
        absorb(sp, 1, True)
    if n_sp > 1:
        with scope("fwd1l"):
            forward(1, (1,))
    def side_block(s, long):
        block = jnp.where(lower == long, sp + away(s), sp - away(s))

        @pl.when((block >= 0) & (block < n_sp) & (block != last))
        def _():
            with scope("absorb"):
                absorb_all(block)

    @pl.loop(1, n_sp)
    def _(s):
        def onward():
            @pl.when(s + 1 < n_sp)
            def _():
                with scope("fwd"):
                    forward(s + 1)

        side_block(s, True)
        if n_sp > 4:
            onward()
        side_block(s, False)
        if n_sp <= 4:
            onward()

    if n_tp == 4:
        @pl.when(dp == 0)
        def _():
            got_extra_far()

    if n_sp > 1:
        with scope("prepare"):
            prepare(last)

    def send_attended(piece, sem):
        def send(d):
            ref = att.at[tp, piece]
            remote(ref, ref, sent.at[6], a_recv.at[sem * d], tp=tp ^ d).start()

        if n_tp == 4:
            send(2)
            for flag, first in ((tp == 1, 1), (tp != 1, 3)):
                @pl.when(flag)
                def _():
                    send(first)
                    send(4 - first)
        else:
            for d in range(1, n_tp):
                send(d)
    lane = lax.broadcasted_iota(jnp.int32, (mid, lanes), 1)
    for half in range(2):
        if n_sp > 1:
            with scope("final"):
                absorb(last, half)
        for g in range(heads // 2):
            even, odd = acc[half, 2 * g], acc[half, 2 * g + 1]
            top = jnp.where(lane < hd, pltpu.roll(even, hd, 1), odd)
            low = jnp.where(lane < hd, even, pltpu.roll(odd, hd, 1))
            att[tp, half, :, g * lanes:(g + 1) * lanes] = (top / low).astype(BF16)
        send_attended(half, half)

    with scope("gotw1"):
        if n_tp == 4:
            @pl.when(dp > 0)
            def _():
                got_extra_far()
        for d in near:
            got_weights(d, 2)
        if near:
            got_across(False)
    copies["wo"].wait()

    def project(group, half, part):
        return dots(att[group, half], wbuf[group, :, part])

    parts = [slice(t * cols, (t + 1) * cols) for t in range(n_tp)]
    tall = [slice(half * mid, (half + 1) * mid) for half in range(2)]
    with scope("own"):
        for half in range(2):
            for part in parts:
                mixed[tall[half], part] = project(tp, half, part)

    with scope("gotw3"):
        if n_tp == 4:
            got_far()
            got_across(True)
        for e in range(1, n_dp):
            if n_tp > 1:
                drain(wbuf.at[:n_tp - 1, :share], f_recv.at[e - 1])
        if n_tp > 1:
            drain(gate_t.at[:n_tp - 1], came.at[3])

    order = [d for d in (1, 3, 2) if d < n_tp]
    for half in range(2):
        for d in order:
            with scope(f"att{half}{d}"):
                if half == 0 and d == order[0]:
                    drain(att.at[:n_tp - 1, 0], a_recv.at[0])
                if half == 1:
                    drain(att.at[tp ^ d, 1], a_recv.at[d])
            if d != order[-1]:
                for part in parts:
                    mixed[tall[half], part] = mixed[tall[half], part] + project(tp ^ d, half, part)
        for t, part in enumerate(parts):
            value = mixed[tall[half], part]
            if order:
                value = value + project(tp ^ order[-1], half, part)
            gate = jnp.concatenate([gate_t[t, j:j + 1, :] for j in range(4)], axis=1)
            out[0, tall[half], part] = (lat[tall[half], part].astype(F32) + gate * value).astype(BF16)

    with scope("sendwait"):
        if n_sp > 1:
            drain(vec_z.at[:n_sp - 1], sent.at[0])
            drain(gate_z.at[:n_sp - 1], sent.at[2])
        if n_tp > 1:
            drain(vec_t.at[:n_tp - 1], sent.at[1])
            drain(gate_t.at[:n_tp - 1], sent.at[3])
            drain(wbuf.at[:n_tp - 1, :share], sent.at[4])
            for e in range(1, n_dp):
                drain(wbuf.at[:n_tp - 1, :share], sent.at[5])
            drain(att.at[:n_tp - 1], sent.at[6])

        if n_sp == 2:
            drain(kvbuf.at[:1], kv_send.at[0])
        if n_sp > 2:
            fewer = (sp == 1).astype(jnp.int32) + (sp == n_sp - 2).astype(jnp.int32)

            @pl.when(edge)
            def _():
                drain(kvbuf.at[:2], kv_send.at[0])

            for less in range(3):
                @pl.when(jnp.logical_not(edge) & (fewer == less))
                def _():
                    drain(kvbuf.at[:min(n_sp, n_sp + 1 - less)], kv_send.at[0])
                    if less == 0:
                        drain(kvbuf.at[:1], kv_send.at[0])


def on_device(
    sizes, latent, condition, context, context_code, shift_weight, scale_weight, gate_weight,
    norm_gain, query_weight, key_weight, value_weight, output_weight, query_gain, key_gain,
    context_bias,
):
    n_sp, n_tp, n_dp = sizes
    rows, width = latent.shape[1:]
    crows = context.shape[1]
    hd = query_gain.shape[0]
    qcols = query_weight.shape[1]
    heads = qcols // hd
    deep, cols = shift_weight.shape
    vmem = pl.BlockSpec(memory_space=pltpu.VMEM)
    hbm = pl.BlockSpec(memory_space=pl.ANY)
    dma = pltpu.SemaphoreType.DMA
    mid = rows // 2
    lanes = 2 * hd
    scratch = [
        pltpu.VMEM((1, deep), BF16), pltpu.VMEM((deep,), BF16), pltpu.VMEM((1, width), F32),
        pltpu.VMEM((1, hd), F32), pltpu.VMEM((1, hd), F32), pltpu.SMEM((heads,), F32),
        pltpu.VMEM((3, deep, cols), BF16),
        pltpu.VMEM((rows, width), BF16),
        pltpu.VMEM((crows, width), BF16),
        pltpu.VMEM((width, qcols), BF16),
        pltpu.VMEM((lanes, width), BF16),
        pltpu.VMEM((width, lanes), BF16),
        pltpu.VMEM((n_tp,) + output_weight.shape, BF16),
        pltpu.VMEM((n_sp, 8, cols // 2), F32),
        pltpu.VMEM((n_tp, 8, cols // 2), F32),
        pltpu.VMEM((n_sp, 4, cols // 4), F32),
        pltpu.VMEM((n_tp, 4, cols // 4), F32),
        pltpu.VMEM((crows, width), BF16),
        pltpu.VMEM((rows, width), BF16),
        pltpu.VMEM((n_sp, crows + rows, lanes), BF16),
        pltpu.VMEM((crows + rows, lanes), BF16),
        pltpu.VMEM((2, heads * mid, lanes), BF16),
        pltpu.VMEM((2, heads, mid, lanes), F32),
        pltpu.VMEM((2, heads, mid, lanes), F32),
        pltpu.VMEM((n_tp, 2, mid, qcols), BF16),
        pltpu.VMEM((rows, width), F32),
        pltpu.VMEM((rows, lanes), F32),
        pltpu.VMEM((rows, lanes), F32),
        pltpu.VMEM((rows, 1), F32),
        dma((8,)), pltpu.SemaphoreType.REGULAR, dma((7,)), dma((5,)),
        dma((1,)), dma((2, n_sp)), dma((2, 4)), dma((3,)), dma((2,)), dma((max(1, n_dp - 1),)), dma((n_tp,)),
    ]
    return pl.pallas_call(
        functools.partial(kernel, sizes),
        out_shape=pltpu.VMEM(latent.shape, BF16),
        in_specs=[hbm] * 15,
        out_specs=vmem,
        scratch_shapes=scratch,
        compiler_params=pltpu.CompilerParams(
            collective_id=0, has_side_effects=True, vmem_limit_bytes=SCOPED_KIB * 1024),
    )(
        condition, context_code, norm_gain[None], query_gain[None], key_gain[None],
        context_bias, latent, context, shift_weight, scale_weight, gate_weight, query_weight,
        key_weight.T, value_weight.T, output_weight,
    )


def solution(mesh):
    sizes = tuple(mesh.shape[axis] for axis in ("sp", "tp", "dp"))
    return jax.shard_map(
        functools.partial(on_device, sizes),
        mesh=mesh,
        in_specs=(
            P("dp", "sp", None),
            P("dp", "sp"),
            P("dp", "sp", None),
            P("sp"),
            P("sp", "tp"),
            P("sp", "tp"),
            P("sp", "tp"),
            P(),
            P(None, "tp"),
            P(None, "tp"),
            P(None, "tp"),
            P("tp", None),
            P(),
            P(),
            P("tp"),
        ),
        out_specs=P("dp", "sp", None),
        check_vma=False,
    )
```

```python
import functools
import math

import jax
import jax.numpy as jnp
from jax import lax
from jax.experimental import pallas as pl
from jax.experimental.pallas import tpu as pltpu
from jax.sharding import PartitionSpec as P

GRID_W = 64
norm_eps = 1e-06
rope_base = 10000.0
F32 = jnp.float32
BF16 = jnp.bfloat16
LANES = 128
LOG2E = math.log2(math.e)
GROUP = 2
SCOPED_KIB = 64384


def tables(first, rows, head_dim):
    quarter = head_dim // 4
    half = head_dim // 2
    shape = (rows, 2 * head_dim)
    token = first + lax.broadcasted_iota(jnp.int32, shape, 0)
    lane = lax.broadcasted_iota(jnp.int32, shape, 1) % head_dim
    pair = lane % half
    index = (pair % quarter).astype(F32)
    place = jnp.where(pair < quarter, token // GRID_W, token % GRID_W).astype(F32)
    angle = place * jnp.exp(index * (-math.log(rope_base) / quarter))
    sine = jnp.sin(angle)
    return jnp.cos(angle), jnp.where(lane < half, -sine, sine)


def kernel(
    sizes,
    condition_h, code_h, gain_h, q_gain_h, k_gain_h, bias_h,
    latent, context, shift_w, scale_w, gate_w, wq, wk, wv, wo,
    out,
    condition, code, gain_ref, q_gain, k_gain, bias_ref,
    modw, lat, ctx, wq_v, wkv, wkv_t, wbuf,
    vec_z, vec_t, gate_z, gate_t, normed_c, normed_l, kvbuf, vals, q_s, m_s, acc, att, mixed, cos_s, sin_s, inv_s,
    local, met, sent, came, kv_send, kv_recv, w_recv, x_recv, s_recv, f_recv, a_recv,
):
    n_sp, n_tp, n_dp = sizes
    sp, tp, dp = lax.axis_index("sp"), lax.axis_index("tp"), lax.axis_index("dp")
    rows, crows = lat.shape[0], ctx.shape[0]
    hd = wk.shape[0]
    qcols = wq_v.shape[1]
    heads = qcols // hd
    width = lat.shape[1]
    cols = width // n_tp
    side = cols // 2
    chip = cols // 4
    mid = rows // 2
    lanes = 2 * hd
    dots = functools.partial(jnp.dot, preferred_element_type=F32)
    dims = (((1,), (1,)), ((), ()))
    scope = jax.named_scope

    barrier = pltpu.get_barrier_semaphore()

    def greet(sem, **where):
        pl.semaphore_signal(sem, inc=1, device_id=where, device_id_type=pl.DeviceIdType.MESH)

    for d in range(1, n_sp):
        greet(barrier, sp=(sp + d) % n_sp)
    for d in range(1, n_tp):
        greet(barrier, tp=tp ^ d)
    for d in range(1, n_dp):
        @pl.when(dp + d < n_dp)
        def _():
            greet(barrier, dp=dp + d)

    copies = {}

    def load(number, name, src, dst):
        copies[name] = pltpu.make_async_copy(src, dst, local.at[number])
        copies[name].start()

    load(0, "condition", condition_h, condition)
    load(1, "code", code_h, code)
    load(2, "m0", shift_w, modw.at[0])
    load(3, "m1", scale_w, modw.at[1])
    load(4, "m2", gate_w, modw.at[2])
    load(5, "ctx", context.at[0], ctx)

    def drain(ref, sem):
        pltpu.make_async_copy(ref, ref, sem).wait()

    def remote(src, dst, s, r, **where):
        return pltpu.make_async_remote_copy(
            src_ref=src, dst_ref=dst, send_sem=s, recv_sem=r,
            device_id=where, device_id_type=pl.DeviceIdType.MESH)

    with scope("modmat"):
        copies["condition"].wait()
        copies["code"].wait()
        load(0, "lat", latent.at[0], lat)
        load(1, "wk", wk, wkv.at[:hd])
        load(1, "wv", wv, wkv.at[hd:])
        row8 = lax.broadcasted_iota(jnp.int32, (8, condition.shape[1]), 0)
        own_code = condition[...].astype(F32)
        shared_code = code[...].astype(F32)[None]
        both = jnp.where(row8 == 0, own_code, jnp.where(row8 == 1, shared_code, 0.0))
        both = (both / (1.0 + jnp.exp(-both))).astype(BF16)
        pieces = []
        for k in range(2):
            copies[f"m{k}"].wait()
            pieces.append(dots(both, modw[k])[:2])
        rows4 = jnp.concatenate(pieces, axis=0)
        vec_z[sp] = jnp.concatenate([rows4[:, :side], rows4[:, side:]], axis=0)

    load(2, "gain", gain_h, gain_ref)
    load(3, "k_gain", k_gain_h, k_gain)

    with scope("barrier"):
        pl.semaphore_wait(barrier, n_sp + n_tp - 2 + dp)

    for d in range(1, n_sp):
        remote(vec_z.at[sp], vec_z.at[sp], sent.at[0], came.at[0], sp=(sp + d) % n_sp).start()
    for d in range(1, n_dp):
        @pl.when(dp - d >= 0)
        def _():
            greet(met, dp=dp - d)

    share = wo.shape[0] // n_dp
    piece = share // 8
    near = [d for d in (1, 2) if d < n_tp]
    paired = n_sp % 2 == 0
    turns = {1: ((3, 1), (4, 2), (0, 3)), 2: ((0, 1), (1, 2), (3, 3))}

    def span(core, first, count):
        return pl.ds(pl.multiple_of(core * share + first * piece, piece), count * piece)

    def extra(core, plane):
        if paired:
            return span(core, 6 + plane % 2, 1)
        return span(core, 6, 2)

    def send_weights(d, turn):
        area = extra(dp, sp) if turn == 3 else span(dp, *turns[d][turn])
        remote(wo.at[area], wbuf.at[tp, area], sent.at[4], w_recv.at[d - 1, turn], tp=tp ^ d).start()

    def share_weights(ref):
        for e in range(1, n_dp):
            remote(ref, ref, sent.at[5], f_recv.at[e - 1], dp=(dp + e) % n_dp).start()

    def got_weights(d, turn):
        ref = wbuf.at[tp ^ d, span(dp, *turns[d][turn])]
        drain(ref, w_recv.at[d - 1, turn])
        if n_tp == 4 and turn < 2:
            remote(ref, ref, sent.at[4], x_recv.at[0], tp=tp ^ (3 - d)).start()
        share_weights(ref)

    def across(d):
        ref = wbuf.at[tp ^ d, extra(dp, sp)]
        if paired:
            remote(ref, ref, sent.at[4], s_recv.at[d // 3], sp=sp ^ 1).start()

    def got_extra():
        for d in near:
            ref = wbuf.at[tp ^ d, extra(dp, sp)]
            drain(ref, w_recv.at[d - 1, 3])
            if n_tp == 4:
                @pl.when(dp % 2 == 2 - d)
                def _():
                    remote(ref, ref, sent.at[4], x_recv.at[1], tp=tp ^ (3 - d)).start()
            across(d)

    def share_extra():
        for d in near:
            share_weights(wbuf.at[tp ^ d, extra(dp, sp)])

    def got_extra_far():
        ref = wbuf.at[tp ^ 3, extra(dp, sp)]
        drain(ref, x_recv.at[1])
        across(3)
        share_weights(ref)

    def got_across(far):
        if paired:
            area = extra(dp, sp + 1)
            those = [3] if far else near
            drain(wbuf.at[:len(those), area], s_recv.at[1 if far else 0])
            for d in those:
                share_weights(wbuf.at[tp ^ d, area])

    def got_far():
        ref = wbuf.at[tp ^ 3, span(dp, 0, 6)]
        drain(ref, x_recv.at[0])
        share_weights(ref)

    for turn in (3, 0):
        for d in near:
            send_weights(d, turn)

    with scope("gate"):
        copies["m2"].wait()
        load(4, "wq", wq, wq_v)
        row = dots(both, modw[2])[:1]
        gate_z[sp] = jnp.concatenate([row[:, j * chip:(j + 1) * chip] for j in range(4)], axis=0)
    for d in range(1, n_sp):
        remote(gate_z.at[sp], gate_z.at[sp], sent.at[2], came.at[2], sp=(sp + d) % n_sp).start()

    with scope("tables"):
        cosine, sine = tables(sp * rows, rows, hd)
        cos_s[...] = cosine
        sin_s[...] = sine
    with scope("inv"):
        copies["ctx"].wait()
        load(5, "wo", wo, wbuf.at[tp])
        floats = ctx[...].astype(F32)
        inv_c = lax.rsqrt(jnp.mean(floats * floats, axis=-1, keepdims=True) + norm_eps)
        copies["lat"].wait()
        floats = lat[...].astype(F32)
        inv_s[...] = lax.rsqrt(jnp.mean(floats * floats, axis=-1, keepdims=True) + norm_eps)

    with scope("turn"):
        drain(wkv, local.at[1])
        for d in range(n_tp):
            wkv_t[d * cols:(d + 1) * cols] = wkv[:, pl.ds(pl.multiple_of((tp ^ d) * cols, cols), cols)].T
    with scope("zwait"):
        if n_sp > 1:
            drain(vec_z.at[:n_sp - 1], came.at[0])
    total = vec_z[0]
    for k in range(1, n_sp):
        total = total + vec_z[k]
    vec_t[tp] = total
    for d in reversed(range(1, n_tp)):
        remote(vec_t.at[tp], vec_t.at[tp], sent.at[1], came.at[1 if d in near else 4], tp=tp ^ d).start()
    with scope("extra"):
        got_extra()
    for turn in (1, 2):
        for d in near:
            send_weights(d, turn)
    early, far = [0] + near, list(range(3, n_tp))
    cut = len(early) * cols

    def modulate(tokens, inverse, which, normed, offsets):
        for d in offsets:
            t = tp ^ d
            for k in range(2):
                part = pl.ds(pl.multiple_of(t * cols + k * side, side), side)
                at = 4 * k + which
                factor = gain_ref[:, part] * (1.0 + vec_t[t, at + 2:at + 3, :])
                shift = vec_t[t, at:at + 1, :]
                values = tokens[:, part].astype(F32) * inverse * factor + shift
                normed[:, d * cols + k * side:d * cols + (k + 1) * side] = values.astype(BF16)

    def kv_copy(block, target, way, part):
        area = pl.ds(0, crows) if part == 0 else pl.ds(crows, rows)
        ref = kvbuf.at[block, area]
        return remote(ref, ref, kv_send.at[0],
                      kv_recv.at[part, lax.rem(block - target - 1 + 2 * n_sp, n_sp)], sp=target)

    def send_own(part):
        @pl.when(sp + 1 < n_sp)
        def _():
            kv_copy(sp, sp + 1, 0, part).start()

        @pl.when(sp > 0)
        def _():
            kv_copy(sp, sp - 1, 1, part).start()

    def send_far(part):
        if n_sp > 2:
            @pl.when(sp == 0)
            def _():
                kv_copy(sp, n_sp - 1, 1, part).start()

            @pl.when(sp == n_sp - 1)
            def _():
                kv_copy(sp, 0, 0, part).start()

    def averages(values):
        n = values.shape[1]
        row = lax.broadcasted_iota(jnp.int32, (n, n), 0) // hd
        col = lax.broadcasted_iota(jnp.int32, (n, n), 1) // hd
        spread = jnp.where(row == col, 1.0 / hd, 0.0).astype(BF16)
        return dots((values * values).astype(BF16), spread)

    def swapped(values):
        lane = lax.broadcasted_iota(jnp.int32, values.shape, 1) % hd
        return jnp.where(lane < hd // 2, pltpu.roll(values, lanes - hd // 2, 1), pltpu.roll(values, hd // 2, 1))

    def key_values(kv, turn):
        lane = lax.broadcasted_iota(jnp.int32, kv.shape, 1)
        keys = kv * lax.rsqrt(averages(kv) + norm_eps) * jnp.concatenate([k_gain[...]] * 2, axis=1)
        if turn:
            keys = keys * cos_s[...] + swapped(keys) * sin_s[...]
        return jnp.where(lane < hd, keys, kv).astype(BF16)

    copies["gain"].wait()
    copies["k_gain"].wait()
    load(2, "q_gain", q_gain_h, q_gain)
    load(3, "bias", bias_h, bias_ref)
    with scope("twait1"):
        if near:
            drain(vec_t.at[:len(near)], came.at[1])
    with scope("modctx"):
        modulate(ctx, inv_c, 1, normed_c, early)
        partial = dots(normed_c[:, :cut], wkv_t[:cut])
        modulate(lat, inv_s[...], 0, normed_l, early)
    with scope("twait2"):
        for d in far:
            drain(vec_t.at[tp ^ d], came.at[4])
    with scope("kvctx"):
        if far:
            modulate(ctx, inv_c, 1, normed_c, far)
            partial = partial + dots(normed_c[:, cut:], wkv_t[cut:])
        kvbuf[sp, :crows] = key_values(partial, False)
    send_far(0)
    send_own(0)

    with scope("kvlat"):
        modulate(lat, inv_s[...], 0, normed_l, far)
        kvbuf[sp, crows:] = key_values(dots(normed_l[...], wkv_t[...]), True)
    send_far(1)
    send_own(1)

    with scope("gotw0"):
        for d in range(1, n_dp):
            @pl.when(dp + d < n_dp)
            def _():
                pl.semaphore_wait(met, 1)
        for d in near:
            got_weights(d, 0)
        share_extra()

    with scope("qproj"):
        copies["wq"].wait()
        copies["q_gain"].wait()
        queries = functools.reduce(jnp.add, [
            dots(normed_l[:, d * cols:(d + 1) * cols], wq_v[pl.ds(pl.multiple_of((tp ^ d) * cols, cols), cols)])
            for d in range(n_tp)])
        factor = lax.rsqrt(averages(queries) + norm_eps)
        gains = jnp.concatenate([q_gain[...]] * 2, axis=1) * (hd ** -0.5 * LOG2E)
        lane = lax.broadcasted_iota(jnp.int32, (rows, lanes), 1)
        for g in range(heads // 2):
            pair = slice(g * lanes, (g + 1) * lanes)
            two = queries[:, pair] * factor[:, pair] * gains
            two = two * cos_s[...] + swapped(two) * sin_s[...]
            for h, one in ((2 * g, two), (2 * g + 1, pltpu.roll(two, hd, 1))):
                one = jnp.where(lane < hd, one, 0.0).astype(BF16)
                for half in range(2):
                    q_s[half, h * mid:(h + 1) * mid] = one[half * mid:(half + 1) * mid]

    with scope("gatez"):
        if n_sp > 1:
            drain(gate_z.at[:n_sp - 1], came.at[2])
        total = gate_z[0]
        for k in range(1, n_sp):
            total = total + gate_z[k]
        gate_t[tp] = total
    for d in range(1, n_tp):
        remote(gate_t.at[tp], gate_t.at[tp], sent.at[3], came.at[3], tp=tp ^ d).start()

    def spread(column, count):
        if count % LANES == 0:
            return jnp.concatenate([column] * (count // LANES), axis=1)
        return column[:, :count]

    def prepare(block):
        pairs = kvbuf[block]
        lane = lax.broadcasted_iota(jnp.int32, pairs.shape, 1)
        vals[...] = jnp.where(lane < hd, jnp.ones_like(pairs), pairs)

    def absorb(block, half, first=False):
        def scores(g):
            query = q_s[half, g * GROUP * mid:(g + 1) * GROUP * mid]
            return (lax.dot_general(query, kvbuf[block, :crows], dims, preferred_element_type=F32),
                    lax.dot_general(query, kvbuf[block, crows:], dims, preferred_element_type=F32))

        ahead = scores(0)
        for g in range(heads // GROUP):
            all_c, all_l = ahead
            if (g + 1) * GROUP < heads:
                ahead = scores(g + 1)
            shares, weights_c, weights_l = [], [], []
            for k in range(GROUP):
                h = g * GROUP + k
                s_c, s_l = all_c[k * mid:(k + 1) * mid], all_l[k * mid:(k + 1) * mid]
                bias = bias_ref[h] * LOG2E
                top = jnp.maximum(s_c.max(axis=1, keepdims=True) + bias, s_l.max(axis=1, keepdims=True))
                top = jnp.broadcast_to(top, (mid, lanes))
                new = top if first else jnp.maximum(m_s[half, h], top)
                weights_c.append(jnp.exp2(s_c - spread(new - bias, crows)).astype(BF16))
                weights_l.append(jnp.exp2(s_l - spread(new, rows)).astype(BF16))
                shares.append(None if first else jnp.exp2(m_s[half, h] - new))
                m_s[half, h] = new
            more = (dots(jnp.concatenate(weights_c, axis=0), vals[:crows])
                    + dots(jnp.concatenate(weights_l, axis=0), vals[crows:]))
            for k in range(GROUP):
                h = g * GROUP + k
                own = more[k * mid:(k + 1) * mid]
                acc[half, h] = own if first else acc[half, h] * shares[k] + own

    def absorb_all(block, first=False):
        prepare(block)

        @pl.loop(0, 2)
        def _(half):
            absorb(block, half, first)

    lower = 2 * sp < n_sp
    edge = (sp == 0) | (sp == n_sp - 1)

    def away(s):
        if n_sp < 3:
            return s
        return jnp.where(edge & (s > 1), jnp.where(s == 2, n_sp - 1, s - 1), s)

    reach = jnp.where(edge, away(n_sp - 1), jnp.where(lower, n_sp - 1 - sp, sp))
    last = jnp.where(lower, sp + reach, sp - reach)

    def passes(block, target):
        if n_sp < 3:
            return (target >= 0) & (target < n_sp)
        far = ((block == 0) & (target == n_sp - 1)) | ((block == n_sp - 1) & (target == 0))
        return (target >= 0) & (target < n_sp) & jnp.logical_not(far)

    def forward(s, parts=(0, 1)):
        d = away(s)
        for part in parts:
            @pl.when(sp - d >= 0)
            def _():
                kv_copy(sp - d, sp, 0, part).wait_recv()

                @pl.when(passes(sp - d, sp + 1))
                def _():
                    kv_copy(sp - d, sp + 1, 0, part).start()

            @pl.when(sp + d < n_sp)
            def _():
                kv_copy(sp + d, sp, 1, part).wait_recv()

                @pl.when(passes(sp + d, sp - 1))
                def _():
                    kv_copy(sp + d, sp - 1, 1, part).start()

    copies["bias"].wait()
    with scope("absorb0"):
        prepare(sp)
        absorb(sp, 0, True)
    with scope("got1"):
        for d in near:
            got_weights(d, 1)
    if n_sp > 1:
        with scope("fwd1c"):
            forward(1, (0,))
    with scope("absorb0"):
        absorb(sp, 1, True)
    if n_sp > 1:
        with scope("fwd1l"):
            forward(1, (1,))
    def side_block(s, long):
        block = jnp.where(lower == long, sp + away(s), sp - away(s))

        @pl.when((block >= 0) & (block < n_sp) & (block != last))
        def _():
            with scope("absorb"):
                absorb_all(block)

    @pl.loop(1, n_sp)
    def _(s):
        def onward():
            @pl.when(s + 1 < n_sp)
            def _():
                with scope("fwd"):
                    forward(s + 1)

        side_block(s, True)
        if n_sp > 4:
            onward()
        side_block(s, False)
        if n_sp <= 4:
            onward()

    if n_tp == 4:
        @pl.when(dp == 0)
        def _():
            got_extra_far()

    if n_sp > 1:
        with scope("prepare"):
            prepare(last)

    def send_attended(piece, sem):
        def send(d):
            ref = att.at[tp, piece]
            remote(ref, ref, sent.at[6], a_recv.at[sem * d], tp=tp ^ d).start()

        if n_tp == 4:
            send(2)
            for flag, first in ((tp == 1, 1), (tp != 1, 3)):
                @pl.when(flag)
                def _():
                    send(first)
                    send(4 - first)
        else:
            for d in range(1, n_tp):
                send(d)
    lane = lax.broadcasted_iota(jnp.int32, (mid, lanes), 1)
    for half in range(2):
        if n_sp > 1:
            with scope("final"):
                absorb(last, half)
        for g in range(heads // 2):
            even, odd = acc[half, 2 * g], acc[half, 2 * g + 1]
            top = jnp.where(lane < hd, pltpu.roll(even, hd, 1), odd)
            low = jnp.where(lane < hd, even, pltpu.roll(odd, hd, 1))
            att[tp, half, :, g * lanes:(g + 1) * lanes] = (top / low).astype(BF16)
        send_attended(half, half)

    with scope("gotw1"):
        if n_tp == 4:
            @pl.when(dp > 0)
            def _():
                got_extra_far()
        for d in near:
            got_weights(d, 2)
        if near:
            got_across(False)
    copies["wo"].wait()

    def project(group, half, part):
        return dots(att[group, half], wbuf[group, :, part])

    parts = [slice(t * cols, (t + 1) * cols) for t in range(n_tp)]
    tall = [slice(half * mid, (half + 1) * mid) for half in range(2)]
    with scope("own"):
        for half in range(2):
            for part in parts:
                mixed[tall[half], part] = project(tp, half, part)

    with scope("gotw3"):
        if n_tp == 4:
            got_far()
            got_across(True)
        for e in range(1, n_dp):
            if n_tp > 1:
                drain(wbuf.at[:n_tp - 1, :share], f_recv.at[e - 1])
        if n_tp > 1:
            drain(gate_t.at[:n_tp - 1], came.at[3])

    order = [d for d in (1, 3, 2) if d < n_tp]
    for half in range(2):
        for d in order:
            with scope(f"att{half}{d}"):
                if half == 0 and d == order[0]:
                    drain(att.at[:n_tp - 1, 0], a_recv.at[0])
                if half == 1:
                    drain(att.at[tp ^ d, 1], a_recv.at[d])
            if d != order[-1]:
                for part in parts:
                    mixed[tall[half], part] = mixed[tall[half], part] + project(tp ^ d, half, part)
        for t, part in enumerate(parts):
            value = mixed[tall[half], part]
            if order:
                value = value + project(tp ^ order[-1], half, part)
            gate = jnp.concatenate([gate_t[t, j:j + 1, :] for j in range(4)], axis=1)
            out[0, tall[half], part] = (lat[tall[half], part].astype(F32) + gate * value).astype(BF16)

    with scope("sendwait"):
        if n_sp > 1:
            drain(vec_z.at[:n_sp - 1], sent.at[0])
            drain(gate_z.at[:n_sp - 1], sent.at[2])
        if n_tp > 1:
            drain(vec_t.at[:n_tp - 1], sent.at[1])
            drain(gate_t.at[:n_tp - 1], sent.at[3])
            drain(wbuf.at[:n_tp - 1, :share], sent.at[4])
            for e in range(1, n_dp):
                drain(wbuf.at[:n_tp - 1, :share], sent.at[5])
            drain(att.at[:n_tp - 1], sent.at[6])

        if n_sp == 2:
            drain(kvbuf.at[:1], kv_send.at[0])
        if n_sp > 2:
            fewer = (sp == 1).astype(jnp.int32) + (sp == n_sp - 2).astype(jnp.int32)

            @pl.when(edge)
            def _():
                drain(kvbuf.at[:2], kv_send.at[0])

            for less in range(3):
                @pl.when(jnp.logical_not(edge) & (fewer == less))
                def _():
                    drain(kvbuf.at[:min(n_sp, n_sp + 1 - less)], kv_send.at[0])
                    if less == 0:
                        drain(kvbuf.at[:1], kv_send.at[0])


def on_device(
    sizes, latent, condition, context, context_code, shift_weight, scale_weight, gate_weight,
    norm_gain, query_weight, key_weight, value_weight, output_weight, query_gain, key_gain,
    context_bias,
):
    n_sp, n_tp, n_dp = sizes
    rows, width = latent.shape[1:]
    crows = context.shape[1]
    hd = query_gain.shape[0]
    qcols = query_weight.shape[1]
    heads = qcols // hd
    deep, cols = shift_weight.shape
    vmem = pl.BlockSpec(memory_space=pltpu.VMEM)
    hbm = pl.BlockSpec(memory_space=pl.ANY)
    dma = pltpu.SemaphoreType.DMA
    mid = rows // 2
    lanes = 2 * hd
    scratch = [
        pltpu.VMEM((1, deep), BF16), pltpu.VMEM((deep,), BF16), pltpu.VMEM((1, width), F32),
        pltpu.VMEM((1, hd), F32), pltpu.VMEM((1, hd), F32), pltpu.SMEM((heads,), F32),
        pltpu.VMEM((3, deep, cols), BF16),
        pltpu.VMEM((rows, width), BF16),
        pltpu.VMEM((crows, width), BF16),
        pltpu.VMEM((width, qcols), BF16),
        pltpu.VMEM((lanes, width), BF16),
        pltpu.VMEM((width, lanes), BF16),
        pltpu.VMEM((n_tp,) + output_weight.shape, BF16),
        pltpu.VMEM((n_sp, 8, cols // 2), F32),
        pltpu.VMEM((n_tp, 8, cols // 2), F32),
        pltpu.VMEM((n_sp, 4, cols // 4), F32),
        pltpu.VMEM((n_tp, 4, cols // 4), F32),
        pltpu.VMEM((crows, width), BF16),
        pltpu.VMEM((rows, width), BF16),
        pltpu.VMEM((n_sp, crows + rows, lanes), BF16),
        pltpu.VMEM((crows + rows, lanes), BF16),
        pltpu.VMEM((2, heads * mid, lanes), BF16),
        pltpu.VMEM((2, heads, mid, lanes), F32),
        pltpu.VMEM((2, heads, mid, lanes), F32),
        pltpu.VMEM((n_tp, 2, mid, qcols), BF16),
        pltpu.VMEM((rows, width), F32),
        pltpu.VMEM((rows, lanes), F32),
        pltpu.VMEM((rows, lanes), F32),
        pltpu.VMEM((rows, 1), F32),
        dma((6,)), pltpu.SemaphoreType.REGULAR, dma((7,)), dma((5,)),
        dma((1,)), dma((2, max(1, n_sp - 1))), dma((2, 4)), dma((2,)), dma((2,)), dma((max(1, n_dp - 1),)), dma((n_tp,)),
    ]
    return pl.pallas_call(
        functools.partial(kernel, sizes),
        out_shape=pltpu.VMEM(latent.shape, BF16),
        in_specs=[hbm] * 15,
        out_specs=vmem,
        scratch_shapes=scratch,
        compiler_params=pltpu.CompilerParams(
            collective_id=0, has_side_effects=True, vmem_limit_bytes=SCOPED_KIB * 1024),
    )(
        condition, context_code, norm_gain[None], query_gain[None], key_gain[None],
        context_bias, latent, context, shift_weight, scale_weight, gate_weight, query_weight,
        key_weight.T, value_weight.T, output_weight,
    )


def solution(mesh):
    sizes = tuple(mesh.shape[axis] for axis in ("sp", "tp", "dp"))
    return jax.shard_map(
        functools.partial(on_device, sizes),
        mesh=mesh,
        in_specs=(
            P("dp", "sp", None),
            P("dp", "sp"),
            P("dp", "sp", None),
            P("sp"),
            P("sp", "tp"),
            P("sp", "tp"),
            P("sp", "tp"),
            P(),
            P(None, "tp"),
            P(None, "tp"),
            P(None, "tp"),
            P("tp", None),
            P(),
            P(),
            P("tp"),
        ),
        out_specs=P("dp", "sp", None),
        check_vma=False,
    )
```
